256 devices in a mesh: kv: 16 (over y, x), tp: 16 (over z, core).
Axes of the slice: x: 4, y: 4, z: 8, core: 2. Of those that a mesh axis runs over, the one named last changes fastest.
Arguments:
- tokens: bfloat16 [128, 4096], P(None, ('kv', 'tp')), may hold values from -41 to 41
- lengths: int32 [128], P('kv'), may hold values from 1 to 8192, 262144 in all
- retention_state: float32 [128, 16, 128, 256], P('kv', 'tp'), may hold values from -4 to 4
- mixer_gain: float32 [4096], P('kv'), may hold values from 0.1 to 1.9
- query_weight: bfloat16 [4096, 2048], P('kv', 'tp'), may hold values from -0.09375 to 0.09375
- key_weight: bfloat16 [4096, 2048], P('kv', 'tp'), may hold values from -0.09375 to 0.09375
- value_weight: bfloat16 [4096, 4096], P('kv', 'tp'), may hold values from -0.09375 to 0.09375
- gate_weight: bfloat16 [4096, 4096], P('kv', 'tp'), may hold values from -0.09375 to 0.09375
- output_weight: bfloat16 [4096, 4096], P('tp', 'kv'), may hold values from -0.125 to 0.125
- channel_gain: float32 [4096], P('kv'), may hold values from 0.1 to 1.9
- ffn_gate: bfloat16 [4096, 11264], P('kv', 'tp'), may hold values from -0.09375 to 0.09375
- ffn_up: bfloat16 [4096, 11264], P('kv', 'tp'), may hold values from -0.09375 to 0.09375
- ffn_down: bfloat16 [11264, 4096], P('tp', 'kv'), may hold values from -0.078125 to 0.078125
Outputs:
- layer_output: bfloat16 [128, 4096], P(None, ('kv', 'tp'))
- new_state: float32 [128, 16, 128, 256], P('kv', 'tp')
The draws below stay inside these ranges and needn't reach their ends.
All inputs are finite; a program needn't handle non-finite values. No bound on the sum of `lengths` on one device may be relied on, other than what follows from the above.
Results may differ from the reference program's by a relative error of at most 0.022.
Values may be sent and summed in bfloat16 or wider, within the bound.
No kernel may reach another device: no remote copies, remote signals or barrier semaphores. Data moves between devices by JAX's collectives and lax.ppermute only.
A program may use at most 64 MiB of HBM per device.

```python
import math
import jax
import jax.numpy as jnp
import numpy as np
from jax import lax

BATCH = 128
D = 4096
HEADS = 16
QK = 128
VD = 256
FF = 11264
MAXLEN = 8192


def draw_tokens(key, part):
    subkeys = jax.random.split(key, 3)
    positions = jnp.arange(D, dtype=jnp.float32) / (D - 1)
    roughness = jnp.exp(jax.random.uniform(subkeys[0], (D,), minval=-0.3, maxval=0.3))
    column_scale = jnp.exp(jnp.log(0.3) + positions * jnp.log(10.0)) * roughness
    base_values = jnp.clip(jax.random.normal(subkeys[2], (BATCH, D)), -5.0, 5.0)
    row_scale = jnp.exp(jax.random.uniform(subkeys[1], (BATCH, 1), minval=jnp.log(0.5), maxval=jnp.log(2.0)))
    return (base_values * row_scale * column_scale[None, :]).astype(jnp.bfloat16)


def with_spikes(entries, stream_key, source, target, parts, factor):
    def block_of(position):
        return (jnp.arange(entries.shape[position]) // (entries.shape[position] // parts)).reshape((-1,) + (1,) * (entries.ndim - 1 - position))

    near = jax.random.permutation(stream_key, parts)[block_of(target)]
    other_side = (block_of(target) + parts // 2) % parts
    return jnp.where((block_of(source) == near) | (block_of(source) == other_side), factor * entries, entries)


def levels(own_key, extent, cuts, low, largest):
    level, own = 1.0, jax.random.fold_in(own_key, 6)
    for dim, shards_of in cuts:
        steps = jnp.exp(jax.random.uniform(jax.random.fold_in(own, dim), (shards_of,), jnp.float32, low / len(cuts), largest / len(cuts)))
        level = level * jnp.repeat(steps, extent[dim] // shards_of).reshape([-1 if axis == dim else 1 for axis in range(len(extent))])
    return level


def split_up(count, total, bound, skew):
    weights = [(1 << 20) // math.isqrt(grade ** skew) + 1 for grade in range(2, count + 1)]
    spare, holding = total - bound - (count - 1), [1] * (count - 1)
    while spare > 0:
        movable = [i for i in range(count - 1) if holding[i] < bound]
        mass, left = sum([weights[i] for i in movable]), spare
        for i in movable:
            more = min(bound - holding[i], max(1, left * weights[i] // mass), spare)
            holding[i] = holding[i] + more
            spare = spare - more
    return np.array([bound] + holding)


def uneven_parts(rng, number_of, total, limit, skew):
    if number_of == 2:
        one = jax.random.randint(rng, (), max(1, total - limit), min(limit, total - 1) + 1)
        return jnp.stack([one, total - one])
    tallies = jnp.asarray(split_up(number_of, total, limit, skew), jnp.int32)
    couples = (number_of - 1) // 2
    source_of, receiver = tallies[1:1 + 2 * couples:2], tallies[2:2 + 2 * couples:2]
    margin = jnp.minimum(source_of - 1, limit - receiver)
    moved = jax.random.randint(jax.random.fold_in(rng, 1), (couples,), 0, 1 << 20) % (margin + 1)
    tallies = tallies.at[1:1 + 2 * couples:2].set(source_of - moved).at[2:2 + 2 * couples:2].set(receiver + moved)
    return tallies[jax.random.permutation(jax.random.fold_in(rng, 2), number_of)]


def centred(rng, extent, width, bound, cuts=(), kind=jnp.bfloat16):
    values = jax.random.normal(rng, extent, jnp.float32) * width
    if len(cuts) > 0:
        values = levels(rng, extent, cuts, -0.22, 0.18) * values
    return jnp.clip(values, min=-bound, max=bound).astype(kind)


def bell_draw_with(stream_key, shape, spread, limit, cuts, heavy, kind=jnp.bfloat16):
    drawn = spread * jax.random.normal(stream_key, shape, jnp.float32)
    if cuts:
        drawn = drawn * levels(stream_key, shape, cuts, -0.22, 0.18)
    return jnp.clip(with_spikes(drawn, jax.random.fold_in(stream_key, 3), *heavy), -limit, limit).astype(kind)


def setup_inputs(seed: int = 0) -> dict:
    streams_of = jax.random.split(jax.random.key(seed), 14)
    return {
        "tokens": draw_tokens(jax.random.fold_in(streams_of[13], 71), 0),
        "lengths": uneven_parts(streams_of[1], BATCH, BATCH * MAXLEN // 4, MAXLEN, 2).astype(jnp.int32),
        "retention_state": centred(streams_of[2], (BATCH, HEADS, QK, VD), 0.3, 4.0, ((0, 16), (1, 16)), jnp.float32),
        "mixer_gain": jnp.clip(1.0 + 0.18 * jax.random.normal(streams_of[3], (D,), jnp.float32), 0.1, 1.9),
        "query_weight": centred(streams_of[4], (D, HEADS * QK), D ** -0.5, 0.09375, ((0, 16), (1, 16))),
        "key_weight": centred(streams_of[5], (D, HEADS * QK), D ** -0.5, 0.09375, ((0, 16), (1, 16))),
        "value_weight": centred(streams_of[6], (D, HEADS * VD), D ** -0.5, 0.09375, ((0, 16), (1, 16))),
        "gate_weight": centred(streams_of[7], (D, HEADS * VD), D ** -0.5, 0.09375, ((0, 16), (1, 16))),
        "output_weight": bell_draw_with(streams_of[8], (HEADS * VD, D), D ** -0.5, 0.125, ((0, 16), (1, 16)), (0, 1, 16, 2.0)),
        "channel_gain": jnp.clip(1.0 + 0.18 * jax.random.normal(streams_of[9], (D,), jnp.float32), 0.1, 1.9),
        "ffn_gate": centred(streams_of[10], (D, FF), D ** -0.5, 0.09375, ((0, 16), (1, 16))),
        "ffn_up": centred(streams_of[11], (D, FF), D ** -0.5, 0.09375, ((0, 16), (1, 16))),
        "ffn_down": bell_draw_with(streams_of[12], (FF, D), FF ** -0.5, 0.078125, ((0, 16), (1, 16)), (0, 1, 16, 2.0)),
    }


def rotate_heads(vectors, positions):
    half_dim = vectors.shape[-1] // 2
    frequency = 10000.0 ** (-jnp.arange(half_dim, dtype=jnp.float32) / half_dim)
    angles = positions.astype(jnp.float32)[:, None, None] * frequency
    cosine = jnp.cos(angles)
    sine_part = jnp.sin(angles)
    first_half = vectors[..., :half_dim]
    second = vectors[..., half_dim:]
    return jnp.concatenate([first_half * cosine - second * sine_part, first_half * sine_part + second * cosine], axis=-1)

def inverse_rms(values):
    return lax.rsqrt(lax.optimization_barrier(jnp.mean(values * values, axis=-1)) + 1e-06)

def reference(tokens, lengths, retention_state, mixer_gain, query_weight, key_weight, value_weight, gate_weight, output_weight, channel_gain, ffn_gate, ffn_up, ffn_down):
    batch_rows = tokens.shape[0]
    tokens_wide = tokens.astype(jnp.float32)
    scale_one = inverse_rms(tokens_wide)[:, None]
    normed = (tokens_wide * mixer_gain).astype(jnp.bfloat16)
    query_proj = jnp.dot(normed, query_weight, preferred_element_type=jnp.float32) * scale_one
    query_rows = rotate_heads(query_proj.reshape(batch_rows, HEADS, QK), lengths).astype(jnp.bfloat16)
    key_proj = jnp.dot(normed, key_weight, preferred_element_type=jnp.float32) * scale_one
    key_rows = (rotate_heads(key_proj.reshape(batch_rows, HEADS, QK), lengths) * QK ** (-0.5)).astype(jnp.bfloat16)
    value_rows = (jnp.dot(normed, value_weight, preferred_element_type=jnp.float32) * scale_one).astype(jnp.bfloat16)
    value_rows = value_rows.reshape(batch_rows, HEADS, VD)
    gate_rows = jnp.dot(normed, gate_weight, preferred_element_type=jnp.float32) * scale_one
    head_ids = jnp.arange(HEADS, dtype=jnp.float32)
    decay_rate = 1.0 - 2.0 ** (-5.0 - 10.0 * head_ids / (HEADS - 1))
    new_state = decay_rate[None, :, None, None] * retention_state + key_rows.astype(jnp.float32)[..., :, None] * value_rows.astype(jnp.float32)[..., None, :]
    retained = jnp.einsum('bhk,bhkv->bhv', query_rows.astype(jnp.float32), new_state, precision=lax.Precision.HIGHEST)
    normalized = retained * inverse_rms(retained)[..., None]
    merged = (normalized.reshape(batch_rows, HEADS * VD) * jax.nn.silu(gate_rows)).astype(jnp.bfloat16)
    residual = (tokens_wide + jnp.dot(merged, output_weight, preferred_element_type=jnp.float32)).astype(jnp.bfloat16)
    residual_wide = residual.astype(jnp.float32)
    scale_two = inverse_rms(residual_wide)[:, None]
    normed_two = (residual_wide * channel_gain).astype(jnp.bfloat16)
    gate_ff = jnp.dot(normed_two, ffn_gate, preferred_element_type=jnp.float32) * scale_two
    up_ff = jnp.dot(normed_two, ffn_up, preferred_element_type=jnp.float32) * scale_two
    hidden = (jax.nn.silu(gate_ff) * up_ff).astype(jnp.bfloat16)
    layer_output = (residual_wide + jnp.dot(hidden, ffn_down, preferred_element_type=jnp.float32)).astype(jnp.bfloat16)
    return (layer_output, new_state)
```

```python
import math

import jax
import jax.numpy as jnp
from jax import lax
from jax.experimental import pallas as pl
from jax.experimental.pallas import tpu as pltpu
from jax.sharding import PartitionSpec as P

D = 4096
HEADS = 16
QK = 128
VD = 256
LANES = 128
F32 = jnp.float32
BF16 = jnp.bfloat16
VMEM_BYTES = 8 << 20
FULL_VMEM_BYTES = 67_043_328 - 1_000_000


def local_call(kernel, outs, *operands, scratch=(), space=pltpu.VMEM, limit=VMEM_BYTES):
    spaces = [space] * len(operands)
    several = isinstance(outs, tuple)
    vmem = pl.BlockSpec(memory_space=pltpu.VMEM)
    return pl.pallas_call(
        kernel,
        out_shape=outs,
        in_specs=[pl.BlockSpec(memory_space=s) for s in spaces],
        out_specs=tuple(vmem for _ in outs) if several else vmem,
        scratch_shapes=scratch,
        compiler_params=pltpu.CompilerParams(vmem_limit_bytes=limit),
    )(*operands)


def shaped(shape, dtype):
    return pltpu.VMEM(shape, dtype)


def store_rows(out_ref, value, start):
    each = out_ref.shape[1]
    for owner in range(out_ref.shape[0]):
        out_ref[owner, :, start : start + value.shape[1]] = value[
            owner * each : (owner + 1) * each
        ].astype(out_ref.dtype)


def all_rows(ref):
    return jnp.concatenate([ref[i].astype(F32) for i in range(ref.shape[0])], axis=0)


def summed(ref):
    total = ref[0].astype(F32)
    for i in range(1, ref.shape[0]):
        total = total + ref[i].astype(F32)
    return total


def prepare(token_ref, length_ref, *refs):
    count = (len(refs) - 6) // 2
    sources, (copies_ref, sine_ref, cosine_ref), fetched = (
        refs[:count],
        refs[count : count + 3],
        refs[count + 3 : 2 * count + 3],
    )
    tokens_vmem, lengths_smem, sems = refs[2 * count + 3 :]
    copies = [
        pltpu.make_async_copy(source, target, sems.at[i])
        for i, (source, target) in enumerate(
            zip((token_ref, length_ref, *sources), (tokens_vmem, lengths_smem, *fetched))
        )
    ]
    for copy in copies:
        copy.start()
    copies[1].wait()
    shape = sine_ref.shape
    row = lax.broadcasted_iota(jnp.int32, shape, 0)
    position = jnp.zeros(shape, F32)
    for i in range(shape[0]):
        position = jnp.where(row == i, lengths_smem[i].astype(F32), position)
    sine, cosine = sine_cosine(position * frequencies(shape))
    first = lax.broadcasted_iota(jnp.int32, shape, 1) < QK // 2
    sine_ref[...] = jnp.where(first, -sine, sine)
    cosine_ref[...] = cosine
    copies[0].wait()
    tokens = tokens_vmem[...]
    for i in range(copies_ref.shape[0]):
        copies_ref[i] = tokens
    for copy in copies[2:]:
        copy.wait()


def project(x_ref, gain_ref, q_ref, k_ref, v_ref, g_ref, out_ref, half_ref):
    x = x_ref[...].astype(F32).reshape(-1, x_ref.shape[2]).T
    normed = (x * gain_ref[...].reshape(1, -1)).astype(BF16)
    at = 0
    for w_ref in (q_ref, k_ref, v_ref, g_ref):
        store_rows(out_ref, jnp.dot(normed, w_ref[...], preferred_element_type=F32), at)
        at += w_ref.shape[1]
    squares = jnp.sum(x * x, axis=1, keepdims=True)
    store_rows(out_ref, jnp.broadcast_to(squares, (x.shape[0], LANES)), at)
    core = lax.rem(lax.axis_index("tp"), 2)
    width = half_ref.shape[1]
    half_ref[...] = jnp.where(core == 0, x[:, :width], x[:, width:]).astype(BF16)


def frequencies(shape):
    lane = lax.broadcasted_iota(jnp.int32, shape, 1)
    result = jnp.ones(shape, F32)
    for bit in range(6):
        factor = 10000.0 ** (-(2.0**bit) / (QK // 2))
        result = jnp.where((lane >> bit) & 1 == 1, result * F32(factor), result)
    return result


def sine_cosine(angle):
    turns = jnp.floor(angle * F32(2.0 / math.pi) + 0.5)
    rest = angle - turns * F32(1.5703125)
    rest = rest - turns * F32(4.837512969970703125e-4)
    rest = rest - turns * F32(7.54978995489188216e-8)
    square = rest * rest
    sine = rest + rest * square * (
        F32(-1.6666654611e-1) + square * (F32(8.3321608736e-3) + square * F32(-1.9515295891e-4))
    )
    cosine = (
        1.0
        - 0.5 * square
        + square
        * square
        * (
            F32(4.166664568298827e-2)
            + square * (F32(-1.388731625493765e-3) + square * F32(2.443315711809948e-5))
        )
    )
    quarter = turns.astype(jnp.int32) & 3
    odd = (quarter & 1) == 1
    first, second = jnp.where(odd, cosine, sine), jnp.where(odd, sine, cosine)
    return (
        jnp.where(quarter >= 2, -first, first),
        jnp.where((quarter == 1) | (quarter == 2), -second, second),
    )


def retain(parts_ref, sine_ref, cosine_ref, state_ref, out_ref, new_ref):
    sums = summed(parts_ref)
    rows = sums.shape[0]
    scale = lax.rsqrt(sums[:, 2 * QK + 2 * VD :] / D + 1e-06)
    wide_scale = jnp.concatenate([scale, scale], axis=1)
    signed, cosine = sine_ref[...], cosine_ref[...]

    def rotated(vectors):
        return vectors * cosine + pltpu.roll(vectors, QK // 2, 1) * signed

    query = rotated(sums[:, :QK] * scale).astype(BF16).astype(F32)
    key = (rotated(sums[:, QK : 2 * QK] * scale) * QK ** (-0.5)).astype(BF16).astype(F32)
    value = (sums[:, 2 * QK : 2 * QK + VD] * wide_scale).astype(BF16).astype(F32)
    gate = sums[:, 2 * QK + VD : 2 * QK + 2 * VD] * wide_scale
    columns = jnp.concatenate([query, key] * (QK // (2 * rows)), axis=0).T
    head = jnp.full((1, VD), lax.axis_index("tp"), jnp.int32).astype(F32)
    decay = 1.0 - jnp.exp2(-5.0 - 10.0 * head / (HEADS - 1))
    retained = []
    for i in range(rows):
        state = (
            decay * state_ref[i, 0]
            + columns[:, rows + i : rows + i + 1] * value[i : i + 1]
        )
        new_ref[i, 0] = state
        retained.append(jnp.sum(state * columns[:, i : i + 1], axis=0, keepdims=True))
    retained = jnp.concatenate(retained, axis=0)
    inverse = lax.rsqrt(jnp.mean(retained * retained, axis=1, keepdims=True) + 1e-06)
    merged = (retained * inverse * (gate / (1.0 + jnp.exp(-gate)))).astype(BF16)
    for i in range(out_ref.shape[0]):
        out_ref[i] = merged


def mix(merged_ref, w_ref, kept_ref, given_ref):
    mixed = jnp.dot(
        all_rows(merged_ref).astype(BF16), w_ref[...], preferred_element_type=F32
    )
    width = kept_ref.shape[1]
    low, high = mixed[:, :width], mixed[:, width:]
    first = lax.rem(lax.axis_index("tp"), 2) == 0
    kept_ref[...] = jnp.where(first, low, high)
    given_ref[...] = jnp.where(first, high, low).astype(BF16)


def add_given(kept_ref, given_ref, out_ref):
    total = (kept_ref[...] + given_ref[...].astype(F32)).astype(BF16)
    for i in range(out_ref.shape[0]):
        out_ref[i] = total


def add_chips(parts_ref, token_ref, out_ref):
    out_ref[...] = (token_ref[...].astype(F32) + summed(parts_ref)).astype(BF16)


def expand(half_ref, other_ref, gain_ref, gate_ref, up_ref, out_ref, mine_ref, flipped_ref):
    me = lax.axis_index("tp")
    first = lax.rem(me, 2) == 0
    half, other = half_ref[...].astype(F32), other_ref[...].astype(F32)
    x = jnp.concatenate(
        [jnp.where(first, half, other), jnp.where(first, other, half)], axis=1
    )
    normed = (x * gain_ref[...].reshape(1, -1)).astype(BF16)
    contract = (((1,), (1,)), ((), ()))
    units = gate_ref.shape[0]
    gate = lax.dot_general(normed, gate_ref[...], contract, preferred_element_type=F32)
    up = lax.dot_general(normed, up_ref[...], contract, preferred_element_type=F32)
    spare = out_ref.shape[2] // 2 - units
    squares = jnp.broadcast_to(jnp.sum(x * x, axis=1, keepdims=True), (x.shape[0], spare))
    store_rows(out_ref, jnp.concatenate([gate, squares, up, squares], axis=1), 0)
    flipped_ref[...] = x.T
    width = mine_ref.shape[0]
    mine_ref[...] = flipped_ref[pl.ds(pl.multiple_of(me * width, width), width), :]


def activate(parts_ref, out_ref):
    sums = summed(parts_ref)
    units, middle = out_ref.shape[2], sums.shape[1] // 2
    scale = lax.rsqrt(sums[:, units : units + 1] / D + 1e-06)
    gate = sums[:, :units] * scale
    up = sums[:, middle : middle + units] * scale
    hidden = (gate / (1.0 + jnp.exp(-gate)) * up).astype(BF16)
    for i in range(out_ref.shape[0]):
        out_ref[i] = hidden


def contract_units(hidden_ref, w_ref, out_ref):
    down = jnp.dot(all_rows(hidden_ref).astype(BF16), w_ref[...], preferred_element_type=F32)
    out_ref[...] = down.T.astype(BF16).reshape(out_ref.shape)


def finish(parts_ref, mine_ref, out_ref):
    out_ref[...] = (mine_ref[...] + summed(parts_ref)).astype(BF16)


def exchanged(blocks, axis, groups=None):
    return lax.all_to_all(blocks, axis, 0, 0, tiled=True, axis_index_groups=groups)


def on_device(
    tokens,
    lengths,
    retention_state,
    mixer_gain,
    query_weight,
    key_weight,
    value_weight,
    gate_weight,
    output_weight,
    channel_gain,
    ffn_gate,
    ffn_up,
    ffn_down,
):
    owners, members = lax.axis_size("kv"), lax.axis_size("tp")
    batch, own_width = tokens.shape
    rows = batch // owners
    block = own_width * members
    half = block // 2
    units = ffn_gate.shape[1]
    middle = -(-(units + 1) // LANES) * LANES
    swap = [(i, i ^ 1) for i in range(members)]
    along_z = [[i + c for i in range(0, members, 2)] for c in range(2)]

    weights = (query_weight, key_weight, value_weight, gate_weight)
    fetch = (mixer_gain, channel_gain, *weights)
    copies, sine, cosine, mixer_gain, channel_gain, *weights = local_call(
        prepare,
        (
            shaped((members, own_width, batch), BF16),
            shaped((rows, QK), F32),
            shaped((rows, QK), F32),
            *(shaped(a.shape, a.dtype) for a in fetch),
        ),
        tokens.T,
        lengths,
        *fetch,
        scratch=(
            pltpu.VMEM((own_width, batch), BF16),
            pltpu.SMEM((rows,), jnp.int32),
            pltpu.SemaphoreType.DMA((len(fetch) + 2,)),
        ),
        space=pltpu.HBM,
        limit=FULL_VMEM_BYTES,
    )
    features = exchanged(copies, "tp")
    width = 2 * QK + 2 * VD + LANES
    parts, token_half = local_call(
        project,
        (shaped((owners, rows, width), BF16), shaped((batch, half), BF16)),
        features,
        mixer_gain,
        *weights,
    )
    merged, new_state = local_call(
        retain,
        (shaped((owners, rows, VD), BF16), shaped(retention_state.shape, F32)),
        exchanged(parts, "kv"),
        sine,
        cosine,
        retention_state,
    )
    kept, given = local_call(
        mix,
        (shaped((batch, half), F32), shaped((batch, half), BF16)),
        exchanged(merged, "kv"),
        output_weight,
    )
    chip_sum = local_call(
        add_given,
        shaped((members // 2, batch, half), BF16),
        kept,
        lax.ppermute(given, "tp", swap),
    )
    residual_half = local_call(
        add_chips,
        shaped((batch, half), BF16),
        exchanged(chip_sum, "tp", along_z),
        token_half,
    )
    parts, mine = local_call(
        expand,
        (shaped((owners, rows, 2 * middle), BF16), shaped((own_width, batch), F32)),
        residual_half,
        lax.ppermute(residual_half, "tp", swap),
        channel_gain,
        ffn_gate.T,
        ffn_up.T,
        scratch=(pltpu.VMEM((block, batch), F32),),
    )
    hidden = local_call(
        activate, shaped((owners, rows, units), BF16), exchanged(parts, "kv")
    )
    down = local_call(
        contract_units,
        shaped((members, own_width, batch), BF16),
        exchanged(hidden, "kv"),
        ffn_down,
    )
    layer_output = local_call(
        finish, jax.ShapeDtypeStruct((own_width, batch), BF16), exchanged(down, "tp"), mine
    )
    return (layer_output.T, new_state)


def solution(mesh):
    in_specs = (
        P(None, ("kv", "tp")),
        P("kv"),
        P("kv", "tp", None, None),
        P("kv"),
        P("kv", "tp"),
        P("kv", "tp"),
        P("kv", "tp"),
        P("kv", "tp"),
        P("tp", "kv"),
        P("kv"),
        P("kv", "tp"),
        P("kv", "tp"),
        P("tp", "kv"),
    )
    out_specs = (P(None, ("kv", "tp")), P("kv", "tp", None, None))
    return jax.shard_map(
        on_device, mesh=mesh, in_specs=in_specs, out_specs=out_specs, check_vma=False
    )
```

```python
import math

import jax
import jax.numpy as jnp
from jax import lax
from jax.experimental import pallas as pl
from jax.experimental.pallas import tpu as pltpu
from jax.sharding import PartitionSpec as P

D = 4096
HEADS = 16
QK = 128
VD = 256
LANES = 128
F32 = jnp.float32
BF16 = jnp.bfloat16
VMEM_BYTES = 8 << 20
FULL_VMEM_BYTES = 67_043_328 - 1_000_000


def local_call(kernel, outs, *operands, scratch=(), space=pltpu.VMEM, out_space=pltpu.VMEM, limit=VMEM_BYTES):
    spaces = [space] * len(operands)
    several = isinstance(outs, tuple)
    vmem = pl.BlockSpec(memory_space=out_space)
    return pl.pallas_call(
        kernel,
        out_shape=outs,
        in_specs=[pl.BlockSpec(memory_space=s) for s in spaces],
        out_specs=tuple(vmem for _ in outs) if several else vmem,
        scratch_shapes=scratch,
        compiler_params=pltpu.CompilerParams(vmem_limit_bytes=limit),
    )(*operands)


def shaped(shape, dtype):
    return pltpu.VMEM(shape, dtype)


def store_rows(out_ref, value, start):
    each = out_ref.shape[1]
    for owner in range(out_ref.shape[0]):
        out_ref[owner, :, start : start + value.shape[1]] = value[
            owner * each : (owner + 1) * each
        ].astype(out_ref.dtype)


def all_rows(ref):
    return jnp.concatenate([ref[i].astype(F32) for i in range(ref.shape[0])], axis=0)


def summed(ref):
    total = ref[0].astype(F32)
    for i in range(1, ref.shape[0]):
        total = total + ref[i].astype(F32)
    return total


def prepare(token_ref, length_ref, *refs):
    count = (len(refs) - 6) // 2
    sources, (copies_ref, sine_ref, cosine_ref), fetched = (
        refs[:count],
        refs[count : count + 3],
        refs[count + 3 : 2 * count + 3],
    )
    tokens_vmem, lengths_smem, sems = refs[2 * count + 3 :]
    copies = [
        pltpu.make_async_copy(source, target, sems.at[i])
        for i, (source, target) in enumerate(
            zip((token_ref, length_ref, *sources), (tokens_vmem, lengths_smem, *fetched))
        )
    ]
    for copy in copies:
        copy.start()
    copies[1].wait()
    shape = sine_ref.shape
    row = lax.broadcasted_iota(jnp.int32, shape, 0)
    position = jnp.zeros(shape, F32)
    for i in range(shape[0]):
        position = jnp.where(row == i, lengths_smem[i].astype(F32), position)
    sine, cosine = sine_cosine(position * frequencies(shape))
    first = lax.broadcasted_iota(jnp.int32, shape, 1) < QK // 2
    sine_ref[...] = jnp.where(first, -sine, sine)
    cosine_ref[...] = cosine
    copies[0].wait()
    tokens = tokens_vmem[...]
    for i in range(copies_ref.shape[0]):
        copies_ref[i] = tokens
    for copy in copies[2:]:
        copy.wait()


def project(x_ref, gain_ref, q_ref, k_ref, v_ref, g_ref, out_ref, half_ref):
    x = x_ref[...].astype(F32).reshape(-1, x_ref.shape[2]).T
    normed = (x * gain_ref[...].reshape(1, -1)).astype(BF16)
    at = 0
    for w_ref in (q_ref, k_ref, v_ref, g_ref):
        store_rows(out_ref, jnp.dot(normed, w_ref[...], preferred_element_type=F32), at)
        at += w_ref.shape[1]
    squares = jnp.sum(x * x, axis=1, keepdims=True)
    store_rows(out_ref, jnp.broadcast_to(squares, (x.shape[0], LANES)), at)
    core = lax.rem(lax.axis_index("tp"), 2)
    width = half_ref.shape[1]
    half_ref[...] = jnp.where(core == 0, x[:, :width], x[:, width:]).astype(BF16)


def frequencies(shape):
    lane = lax.broadcasted_iota(jnp.int32, shape, 1)
    result = jnp.ones(shape, F32)
    for bit in range(6):
        factor = 10000.0 ** (-(2.0**bit) / (QK // 2))
        result = jnp.where((lane >> bit) & 1 == 1, result * F32(factor), result)
    return result


def sine_cosine(angle):
    turns = jnp.floor(angle * F32(2.0 / math.pi) + 0.5)
    rest = angle - turns * F32(1.5703125)
    rest = rest - turns * F32(4.837512969970703125e-4)
    rest = rest - turns * F32(7.54978995489188216e-8)
    square = rest * rest
    sine = rest + rest * square * (
        F32(-1.6666654611e-1) + square * (F32(8.3321608736e-3) + square * F32(-1.9515295891e-4))
    )
    cosine = (
        1.0
        - 0.5 * square
        + square
        * square
        * (
            F32(4.166664568298827e-2)
            + square * (F32(-1.388731625493765e-3) + square * F32(2.443315711809948e-5))
        )
    )
    quarter = turns.astype(jnp.int32) & 3
    odd = (quarter & 1) == 1
    first, second = jnp.where(odd, cosine, sine), jnp.where(odd, sine, cosine)
    return (
        jnp.where(quarter >= 2, -first, first),
        jnp.where((quarter == 1) | (quarter == 2), -second, second),
    )


def retain(parts_ref, sine_ref, cosine_ref, state_ref, out_ref, new_ref):
    sums = summed(parts_ref)
    rows = sums.shape[0]
    scale = lax.rsqrt(sums[:, 2 * QK + 2 * VD :] / D + 1e-06)
    wide_scale = jnp.concatenate([scale, scale], axis=1)
    signed, cosine = sine_ref[...], cosine_ref[...]

    def rotated(vectors):
        return vectors * cosine + pltpu.roll(vectors, QK // 2, 1) * signed

    query = rotated(sums[:, :QK] * scale).astype(BF16).astype(F32)
    key = (rotated(sums[:, QK : 2 * QK] * scale) * QK ** (-0.5)).astype(BF16).astype(F32)
    value = (sums[:, 2 * QK : 2 * QK + VD] * wide_scale).astype(BF16).astype(F32)
    gate = sums[:, 2 * QK + VD : 2 * QK + 2 * VD] * wide_scale
    columns = jnp.concatenate([query, key] * (QK // (2 * rows)), axis=0).T
    head = jnp.full((1, VD), lax.axis_index("tp"), jnp.int32).astype(F32)
    decay = 1.0 - jnp.exp2(-5.0 - 10.0 * head / (HEADS - 1))
    retained = []
    for i in range(rows):
        state = (
            decay * state_ref[i, 0]
            + columns[:, rows + i : rows + i + 1] * value[i : i + 1]
        )
        new_ref[i, 0] = state
        retained.append(jnp.sum(state * columns[:, i : i + 1], axis=0, keepdims=True))
    retained = jnp.concatenate(retained, axis=0)
    inverse = lax.rsqrt(jnp.mean(retained * retained, axis=1, keepdims=True) + 1e-06)
    merged = (retained * inverse * (gate / (1.0 + jnp.exp(-gate)))).astype(BF16)
    for i in range(out_ref.shape[0]):
        out_ref[i] = merged


def write_out(value_ref, out_ref, sem):
    copy = pltpu.make_async_copy(value_ref, out_ref, sem)
    copy.start()
    copy.wait()


def mix(merged_ref, w_ref, kept_ref, given_ref):
    mixed = jnp.dot(
        all_rows(merged_ref).astype(BF16), w_ref[...], preferred_element_type=F32
    )
    width = kept_ref.shape[1]
    low, high = mixed[:, :width], mixed[:, width:]
    first = lax.rem(lax.axis_index("tp"), 2) == 0
    kept_ref[...] = jnp.where(first, low, high)
    given_ref[...] = jnp.where(first, high, low).astype(BF16)


def add_given(kept_ref, given_ref, out_ref):
    total = (kept_ref[...] + given_ref[...].astype(F32)).astype(BF16)
    for i in range(out_ref.shape[0]):
        out_ref[i] = total


def add_chips(parts_ref, token_ref, out_ref):
    out_ref[...] = (token_ref[...].astype(F32) + summed(parts_ref)).astype(BF16)


def expand(half_ref, other_ref, gain_ref, gate_ref, up_ref, out_ref, mine_ref, flipped_ref):
    me = lax.axis_index("tp")
    first = lax.rem(me, 2) == 0
    half, other = half_ref[...].astype(F32), other_ref[...].astype(F32)
    x = jnp.concatenate(
        [jnp.where(first, half, other), jnp.where(first, other, half)], axis=1
    )
    normed = (x * gain_ref[...].reshape(1, -1)).astype(BF16)
    contract = (((1,), (1,)), ((), ()))
    units = gate_ref.shape[0]
    gate = lax.dot_general(normed, gate_ref[...], contract, preferred_element_type=F32)
    up = lax.dot_general(normed, up_ref[...], contract, preferred_element_type=F32)
    spare = out_ref.shape[2] // 2 - units
    squares = jnp.broadcast_to(jnp.sum(x * x, axis=1, keepdims=True), (x.shape[0], spare))
    store_rows(out_ref, jnp.concatenate([gate, squares, up, squares], axis=1), 0)
    flipped_ref[...] = x.T
    width = mine_ref.shape[0]
    mine_ref[...] = flipped_ref[pl.ds(pl.multiple_of(me * width, width), width), :]


def activate(parts_ref, out_ref):
    sums = summed(parts_ref)
    units, middle = out_ref.shape[2], sums.shape[1] // 2
    scale = lax.rsqrt(sums[:, units : units + 1] / D + 1e-06)
    gate = sums[:, :units] * scale
    up = sums[:, middle : middle + units] * scale
    hidden = (gate / (1.0 + jnp.exp(-gate)) * up).astype(BF16)
    for i in range(out_ref.shape[0]):
        out_ref[i] = hidden


def contract_units(hidden_ref, w_ref, out_ref):
    down = jnp.dot(all_rows(hidden_ref).astype(BF16), w_ref[...], preferred_element_type=F32)
    out_ref[...] = down.T.astype(BF16).reshape(out_ref.shape)


def finish(parts_ref, mine_ref, out_ref):
    out_ref[...] = (mine_ref[...] + summed(parts_ref)).astype(BF16)


def exchanged(blocks, axis, groups=None):
    return lax.all_to_all(blocks, axis, 0, 0, tiled=True, axis_index_groups=groups)


def on_device(
    tokens,
    lengths,
    retention_state,
    mixer_gain,
    query_weight,
    key_weight,
    value_weight,
    gate_weight,
    output_weight,
    channel_gain,
    ffn_gate,
    ffn_up,
    ffn_down,
):
    owners, members = lax.axis_size("kv"), lax.axis_size("tp")
    batch, own_width = tokens.shape
    rows = batch // owners
    block = own_width * members
    half = block // 2
    units = ffn_gate.shape[1]
    middle = -(-(units + 1) // LANES) * LANES
    swap = [(i, i ^ 1) for i in range(members)]
    along_z = [[i + c for i in range(0, members, 2)] for c in range(2)]

    weights = (query_weight, key_weight, value_weight, gate_weight)
    fetch = (mixer_gain, channel_gain, *weights)
    copies, sine, cosine, mixer_gain, channel_gain, *weights = local_call(
        prepare,
        (
            shaped((members, own_width, batch), BF16),
            shaped((rows, QK), F32),
            shaped((rows, QK), F32),
            *(shaped(a.shape, a.dtype) for a in fetch),
        ),
        tokens.T,
        lengths,
        *fetch,
        scratch=(
            pltpu.VMEM((own_width, batch), BF16),
            pltpu.SMEM((rows,), jnp.int32),
            pltpu.SemaphoreType.DMA((len(fetch) + 2,)),
        ),
        space=pltpu.HBM,
        limit=FULL_VMEM_BYTES,
    )
    features = exchanged(copies, "tp")
    width = 2 * QK + 2 * VD + LANES
    parts, token_half = local_call(
        project,
        (shaped((owners, rows, width), BF16), shaped((batch, half), BF16)),
        features,
        mixer_gain,
        *weights,
    )
    merged, new_state = local_call(
        retain,
        (shaped((owners, rows, VD), BF16), shaped(retention_state.shape, F32)),
        exchanged(parts, "kv"),
        sine,
        cosine,
        retention_state,
    )
    kept, given = local_call(
        mix,
        (shaped((batch, half), F32), shaped((batch, half), BF16)),
        exchanged(merged, "kv"),
        output_weight,
    )
    swapped = lax.ppermute(given, "tp", swap)
    new_state, _ = lax.optimization_barrier((new_state, given))
    new_state = local_call(
        write_out,
        jax.ShapeDtypeStruct(retention_state.shape, F32),
        new_state,
        scratch=(pltpu.SemaphoreType.DMA,),
        out_space=pl.ANY,
    )
    swapped, new_state = lax.optimization_barrier((swapped, new_state))
    chip_sum = local_call(
        add_given, shaped((members // 2, batch, half), BF16), kept, swapped
    )
    residual_half = local_call(
        add_chips,
        shaped((batch, half), BF16),
        exchanged(chip_sum, "tp", along_z),
        token_half,
    )
    parts, mine = local_call(
        expand,
        (shaped((owners, rows, 2 * middle), BF16), shaped((own_width, batch), F32)),
        residual_half,
        lax.ppermute(residual_half, "tp", swap),
        channel_gain,
        ffn_gate.T,
        ffn_up.T,
        scratch=(pltpu.VMEM((block, batch), F32),),
    )
    hidden = local_call(
        activate, shaped((owners, rows, units), BF16), exchanged(parts, "kv")
    )
    down = local_call(
        contract_units,
        shaped((members, own_width, batch), BF16),
        exchanged(hidden, "kv"),
        ffn_down,
    )
    layer_output = local_call(
        finish, jax.ShapeDtypeStruct((own_width, batch), BF16), exchanged(down, "tp"), mine
    )
    return (layer_output.T, new_state)


def solution(mesh):
    in_specs = (
        P(None, ("kv", "tp")),
        P("kv"),
        P("kv", "tp", None, None),
        P("kv"),
        P("kv", "tp"),
        P("kv", "tp"),
        P("kv", "tp"),
        P("kv", "tp"),
        P("tp", "kv"),
        P("kv"),
        P("kv", "tp"),
        P("kv", "tp"),
        P("tp", "kv"),
    )
    out_specs = (P(None, ("kv", "tp")), P("kv", "tp", None, None))
    return jax.shard_map(
        on_device, mesh=mesh, in_specs=in_specs, out_specs=out_specs, check_vma=False
    )
```

```python
import math

import jax
import jax.numpy as jnp
from jax import lax
from jax.experimental import pallas as pl
from jax.experimental.pallas import tpu as pltpu
from jax.sharding import Mesh, PartitionSpec as P

D = 4096
HEADS = 16
QK = 128
VD = 256
LANES = 128
F32 = jnp.float32
BF16 = jnp.bfloat16
VMEM_BYTES = 8 << 20
FULL_VMEM_BYTES = 67_043_328 - 1_000_000


def local_call(kernel, outs, *operands, scratch=(), space=pltpu.VMEM, out_space=pltpu.VMEM, limit=VMEM_BYTES):
    spaces = [space] * len(operands)
    several = isinstance(outs, tuple)
    vmem = pl.BlockSpec(memory_space=out_space)
    return pl.pallas_call(
        kernel,
        out_shape=outs,
        in_specs=[pl.BlockSpec(memory_space=s) for s in spaces],
        out_specs=tuple(vmem for _ in outs) if several else vmem,
        scratch_shapes=scratch,
        compiler_params=pltpu.CompilerParams(vmem_limit_bytes=limit),
    )(*operands)


def tp_index():
    return lax.axis_index("z") * lax.axis_size("core") + lax.axis_index("core")


def shaped(shape, dtype):
    return pltpu.VMEM(shape, dtype)


def store_rows(out_ref, value, start):
    each = out_ref.shape[1]
    for owner in range(out_ref.shape[0]):
        out_ref[owner, :, start : start + value.shape[1]] = value[
            owner * each : (owner + 1) * each
        ].astype(out_ref.dtype)


def all_rows(ref):
    return jnp.concatenate([ref[i].astype(F32) for i in range(ref.shape[0])], axis=0)


def summed(ref):
    total = ref[0].astype(F32)
    for i in range(1, ref.shape[0]):
        total = total + ref[i].astype(F32)
    return total


def prepare(token_ref, length_ref, *refs):
    count = (len(refs) - 6) // 2
    sources, (copies_ref, sine_ref, cosine_ref), fetched = (
        refs[:count],
        refs[count : count + 3],
        refs[count + 3 : 2 * count + 3],
    )
    tokens_vmem, lengths_smem, sems = refs[2 * count + 3 :]
    copies = [
        pltpu.make_async_copy(source, target, sems.at[i])
        for i, (source, target) in enumerate(
            zip((token_ref, length_ref, *sources), (tokens_vmem, lengths_smem, *fetched))
        )
    ]
    for copy in copies:
        copy.start()
    copies[1].wait()
    shape = sine_ref.shape
    row = lax.broadcasted_iota(jnp.int32, shape, 0)
    position = jnp.zeros(shape, F32)
    for i in range(shape[0]):
        position = jnp.where(row == i, lengths_smem[i].astype(F32), position)
    sine, cosine = sine_cosine(position * frequencies(shape))
    first = lax.broadcasted_iota(jnp.int32, shape, 1) < QK // 2
    sine_ref[...] = jnp.where(first, -sine, sine)
    cosine_ref[...] = cosine
    copies[0].wait()
    tokens = tokens_vmem[...]
    for i in range(copies_ref.shape[0]):
        copies_ref[i] = tokens
    for copy in copies[2:]:
        copy.wait()


def project(x_ref, gain_ref, q_ref, k_ref, v_ref, g_ref, out_ref, half_ref):
    x = x_ref[...].astype(F32).reshape(-1, x_ref.shape[2]).T
    normed = (x * gain_ref[...].reshape(1, -1)).astype(BF16)
    at = 0
    for w_ref in (q_ref, k_ref, v_ref, g_ref):
        store_rows(out_ref, jnp.dot(normed, w_ref[...], preferred_element_type=F32), at)
        at += w_ref.shape[1]
    squares = jnp.sum(x * x, axis=1, keepdims=True)
    store_rows(out_ref, jnp.broadcast_to(squares, (x.shape[0], LANES)), at)
    core = lax.axis_index("core")
    width = half_ref.shape[1]
    half_ref[...] = jnp.where(core == 0, x[:, :width], x[:, width:]).astype(BF16)


def frequencies(shape):
    lane = lax.broadcasted_iota(jnp.int32, shape, 1)
    result = jnp.ones(shape, F32)
    for bit in range(6):
        factor = 10000.0 ** (-(2.0**bit) / (QK // 2))
        result = jnp.where((lane >> bit) & 1 == 1, result * F32(factor), result)
    return result


def sine_cosine(angle):
    turns = jnp.floor(angle * F32(2.0 / math.pi) + 0.5)
    rest = angle - turns * F32(1.5703125)
    rest = rest - turns * F32(4.837512969970703125e-4)
    rest = rest - turns * F32(7.54978995489188216e-8)
    square = rest * rest
    sine = rest + rest * square * (
        F32(-1.6666654611e-1) + square * (F32(8.3321608736e-3) + square * F32(-1.9515295891e-4))
    )
    cosine = (
        1.0
        - 0.5 * square
        + square
        * square
        * (
            F32(4.166664568298827e-2)
            + square * (F32(-1.388731625493765e-3) + square * F32(2.443315711809948e-5))
        )
    )
    quarter = turns.astype(jnp.int32) & 3
    odd = (quarter & 1) == 1
    first, second = jnp.where(odd, cosine, sine), jnp.where(odd, sine, cosine)
    return (
        jnp.where(quarter >= 2, -first, first),
        jnp.where((quarter == 1) | (quarter == 2), -second, second),
    )


def retain(parts_ref, sine_ref, cosine_ref, state_ref, out_ref, new_ref):
    sums = summed(parts_ref)
    rows = sums.shape[0]
    scale = lax.rsqrt(sums[:, 2 * QK + 2 * VD :] / D + 1e-06)
    wide_scale = jnp.concatenate([scale, scale], axis=1)
    signed, cosine = sine_ref[...], cosine_ref[...]

    def rotated(vectors):
        return vectors * cosine + pltpu.roll(vectors, QK // 2, 1) * signed

    query = rotated(sums[:, :QK] * scale).astype(BF16).astype(F32)
    key = (rotated(sums[:, QK : 2 * QK] * scale) * QK ** (-0.5)).astype(BF16).astype(F32)
    value = (sums[:, 2 * QK : 2 * QK + VD] * wide_scale).astype(BF16).astype(F32)
    gate = sums[:, 2 * QK + VD : 2 * QK + 2 * VD] * wide_scale
    columns = jnp.concatenate([query, key] * (QK // (2 * rows)), axis=0).T
    head = jnp.full((1, VD), tp_index(), jnp.int32).astype(F32)
    decay = 1.0 - jnp.exp2(-5.0 - 10.0 * head / (HEADS - 1))
    retained = []
    for i in range(rows):
        state = (
            decay * state_ref[i, 0]
            + columns[:, rows + i : rows + i + 1] * value[i : i + 1]
        )
        new_ref[i, 0] = state
        retained.append(jnp.sum(state * columns[:, i : i + 1], axis=0, keepdims=True))
    retained = jnp.concatenate(retained, axis=0)
    inverse = lax.rsqrt(jnp.mean(retained * retained, axis=1, keepdims=True) + 1e-06)
    merged = (retained * inverse * (gate / (1.0 + jnp.exp(-gate)))).astype(BF16)
    for i in range(out_ref.shape[0]):
        out_ref[i] = merged


def write_out(value_ref, out_ref, sem):
    copy = pltpu.make_async_copy(value_ref, out_ref, sem)
    copy.start()
    copy.wait()


def mix(merged_ref, own_ref, other_ref, out_ref):
    core = lax.axis_index("core")
    half = out_ref.shape[2]
    total = None
    for w_ref, which in ((own_ref, core), (other_ref, 1 - core)):
        merged = jnp.concatenate(
            [merged_ref[i + which].astype(F32) for i in range(0, merged_ref.shape[0], 2)], axis=0
        )
        weight = jnp.where(core == 0, w_ref[:, :half], w_ref[:, half:])
        part = jnp.dot(merged.astype(BF16), weight, preferred_element_type=F32)
        total = part if total is None else total + part
    total = total.astype(BF16)
    for i in range(out_ref.shape[0]):
        out_ref[i] = total


def add_chips(parts_ref, token_ref, out_ref):
    out_ref[...] = (token_ref[...].astype(F32) + summed(parts_ref)).astype(BF16)


def expand(half_ref, other_ref, gain_ref, gate_ref, up_ref, out_ref, mine_ref, flipped_ref):
    me = tp_index()
    first = lax.axis_index("core") == 0
    half, other = half_ref[...].astype(F32), other_ref[...].astype(F32)
    x = jnp.concatenate(
        [jnp.where(first, half, other), jnp.where(first, other, half)], axis=1
    )
    normed = (x * gain_ref[...].reshape(1, -1)).astype(BF16)
    contract = (((1,), (1,)), ((), ()))
    units = gate_ref.shape[0]
    gate = lax.dot_general(normed, gate_ref[...], contract, preferred_element_type=F32)
    up = lax.dot_general(normed, up_ref[...], contract, preferred_element_type=F32)
    spare = out_ref.shape[2] // 2 - units
    squares = jnp.broadcast_to(jnp.sum(x * x, axis=1, keepdims=True), (x.shape[0], spare))
    store_rows(out_ref, jnp.concatenate([gate, squares, up, squares], axis=1), 0)
    flipped_ref[...] = x.T
    width = mine_ref.shape[0]
    mine_ref[...] = flipped_ref[pl.ds(pl.multiple_of(me * width, width), width), :]


def activate(parts_ref, out_ref):
    sums = summed(parts_ref)
    units, middle = out_ref.shape[2], sums.shape[1] // 2
    scale = lax.rsqrt(sums[:, units : units + 1] / D + 1e-06)
    gate = sums[:, :units] * scale
    up = sums[:, middle : middle + units] * scale
    hidden = (gate / (1.0 + jnp.exp(-gate)) * up).astype(BF16)
    for i in range(out_ref.shape[0]):
        out_ref[i] = hidden


def contract_units(hidden_ref, w_ref, out_ref):
    down = jnp.dot(all_rows(hidden_ref).astype(BF16), w_ref[...], preferred_element_type=F32)
    out_ref[...] = down.T.astype(BF16).reshape(out_ref.shape)


def finish(parts_ref, mine_ref, out_ref):
    out_ref[...] = (mine_ref[...] + summed(parts_ref)).astype(BF16)


def exchanged(blocks, axis, groups=None):
    return lax.all_to_all(blocks, axis, 0, 0, tiled=True, axis_index_groups=groups)


def on_device(
    tokens,
    lengths,
    retention_state,
    mixer_gain,
    query_weight,
    key_weight,
    value_weight,
    gate_weight,
    output_weight,
    channel_gain,
    ffn_gate,
    ffn_up,
    ffn_down,
):
    owners, chips, cores = (lax.axis_size(a) for a in ("kv", "z", "core"))
    members = chips * cores
    batch, own_width = tokens.shape
    rows = batch // owners
    block = own_width * members
    half = block // 2
    units = ffn_gate.shape[1]
    middle = -(-(units + 1) // LANES) * LANES
    swap = [(0, 1), (1, 0)]
    along_z = [[3 * i % chips for i in range(chips)]]

    weights = (query_weight, key_weight, value_weight, gate_weight)
    fetch = (mixer_gain, channel_gain, *weights)
    copies, sine, cosine, mixer_gain, channel_gain, *weights = local_call(
        prepare,
        (
            shaped((members, own_width, batch), BF16),
            shaped((rows, QK), F32),
            shaped((rows, QK), F32),
            *(shaped(a.shape, a.dtype) for a in fetch),
        ),
        tokens.T,
        lengths,
        *fetch,
        scratch=(
            pltpu.VMEM((own_width, batch), BF16),
            pltpu.SMEM((rows,), jnp.int32),
            pltpu.SemaphoreType.DMA((len(fetch) + 2,)),
        ),
        space=pltpu.HBM,
        limit=FULL_VMEM_BYTES,
    )
    other_weight = lax.ppermute(output_weight, "core", swap)
    features = exchanged(copies, ("z", "core"))
    features, other_weight = lax.optimization_barrier((features, other_weight))
    width = 2 * QK + 2 * VD + LANES
    parts, token_half = local_call(
        project,
        (shaped((owners, rows, width), BF16), shaped((batch, half), BF16)),
        features,
        mixer_gain,
        *weights,
    )
    merged, new_state = local_call(
        retain,
        (shaped((owners * cores, rows, VD), BF16), shaped(retention_state.shape, F32)),
        exchanged(parts, "kv"),
        sine,
        cosine,
        retention_state,
    )
    chip_sum = local_call(
        mix,
        shaped((chips, batch, half), BF16),
        exchanged(merged, ("kv", "core")),
        output_weight,
        other_weight,
    )
    residual_half = local_call(
        add_chips,
        shaped((batch, half), BF16),
        exchanged(chip_sum, "z", along_z),
        token_half,
    )
    residual_other = lax.ppermute(residual_half, "core", swap)
    new_state, _ = lax.optimization_barrier((new_state, residual_half))
    new_state = local_call(
        write_out,
        jax.ShapeDtypeStruct(retention_state.shape, F32),
        new_state,
        scratch=(pltpu.SemaphoreType.DMA,),
        out_space=pl.ANY,
    )
    residual_other, new_state = lax.optimization_barrier((residual_other, new_state))
    parts, mine = local_call(
        expand,
        (shaped((owners, rows, 2 * middle), BF16), shaped((own_width, batch), F32)),
        residual_half,
        residual_other,
        channel_gain,
        ffn_gate.T,
        ffn_up.T,
        scratch=(pltpu.VMEM((block, batch), F32),),
    )
    hidden = local_call(
        activate, shaped((owners, rows, units), BF16), exchanged(parts, "kv")
    )
    down = local_call(
        contract_units,
        shaped((members, own_width, batch), BF16),
        exchanged(hidden, "kv"),
        ffn_down,
    )
    layer_output = local_call(
        finish, jax.ShapeDtypeStruct((own_width, batch), BF16), exchanged(down, ("z", "core")), mine
    )
    return (layer_output.T, new_state)


def solution(mesh):
    split = Mesh(
        mesh.devices.reshape(mesh.shape["kv"], mesh.shape["tp"] // 2, 2), ("kv", "z", "core")
    )
    tp = ("z", "core")
    in_specs = (
        P(None, ("kv", *tp)),
        P("kv"),
        P("kv", tp, None, None),
        P("kv"),
        P("kv", tp),
        P("kv", tp),
        P("kv", tp),
        P("kv", tp),
        P(tp, "kv"),
        P("kv"),
        P("kv", tp),
        P("kv", tp),
        P(tp, "kv"),
    )
    out_specs = (P(None, ("kv", *tp)), P("kv", tp, None, None))
    return jax.shard_map(
        on_device, mesh=split, in_specs=in_specs, out_specs=out_specs, check_vma=False
    )
```

```python
import math

import jax
import jax.numpy as jnp
from jax import lax
from jax.experimental import pallas as pl
from jax.experimental.pallas import tpu as pltpu
from jax.sharding import Mesh, PartitionSpec as P

D = 4096
HEADS = 16
QK = 128
VD = 256
LANES = 128
KV_ORDER = (0, 8, 15, 14, 5, 2, 3, 11, 6, 13, 10, 4, 9, 7, 1, 12)
F32 = jnp.float32
BF16 = jnp.bfloat16
VMEM_BYTES = 8 << 20
FULL_VMEM_BYTES = 67_043_328 - 1_000_000


def local_call(kernel, outs, *operands, scratch=(), space=pltpu.VMEM, out_space=pltpu.VMEM, limit=VMEM_BYTES):
    spaces = [space] * len(operands)
    several = isinstance(outs, tuple)
    vmem = pl.BlockSpec(memory_space=out_space)
    return pl.pallas_call(
        kernel,
        out_shape=outs,
        in_specs=[pl.BlockSpec(memory_space=s) for s in spaces],
        out_specs=tuple(vmem for _ in outs) if several else vmem,
        scratch_shapes=scratch,
        compiler_params=pltpu.CompilerParams(vmem_limit_bytes=limit),
    )(*operands)


def tp_index():
    return lax.axis_index("z") * lax.axis_size("core") + lax.axis_index("core")


def shaped(shape, dtype):
    return pltpu.VMEM(shape, dtype)


def kv_order(owners):
    return KV_ORDER if owners == len(KV_ORDER) else tuple(range(owners))


def store_rows(out_ref, value, start):
    each = out_ref.shape[1]
    for at, owner in enumerate(kv_order(out_ref.shape[0])):
        out_ref[at, :, start : start + value.shape[1]] = value[
            owner * each : (owner + 1) * each
        ].astype(out_ref.dtype)


def all_rows(ref):
    order = kv_order(ref.shape[0])
    return jnp.concatenate(
        [ref[order.index(owner)].astype(F32) for owner in range(ref.shape[0])], axis=0
    )


def summed(ref):
    total = ref[0].astype(F32)
    for i in range(1, ref.shape[0]):
        total = total + ref[i].astype(F32)
    return total


def prepare(token_ref, length_ref, *refs):
    count = (len(refs) - 6) // 2
    sources, (copies_ref, sine_ref, cosine_ref), fetched = (
        refs[:count],
        refs[count : count + 3],
        refs[count + 3 : 2 * count + 3],
    )
    tokens_vmem, lengths_smem, sems = refs[2 * count + 3 :]
    copies = [
        pltpu.make_async_copy(source, target, sems.at[i])
        for i, (source, target) in enumerate(
            zip((token_ref, length_ref, *sources), (tokens_vmem, lengths_smem, *fetched))
        )
    ]
    for copy in copies:
        copy.start()
    copies[1].wait()
    shape = sine_ref.shape
    row = lax.broadcasted_iota(jnp.int32, shape, 0)
    position = jnp.zeros(shape, F32)
    for i in range(shape[0]):
        position = jnp.where(row == i, lengths_smem[i].astype(F32), position)
    sine, cosine = sine_cosine(position * frequencies(shape))
    first = lax.broadcasted_iota(jnp.int32, shape, 1) < QK // 2
    sine_ref[...] = jnp.where(first, -sine, sine)
    cosine_ref[...] = cosine
    copies[0].wait()
    tokens = tokens_vmem[...]
    for i in range(copies_ref.shape[0]):
        copies_ref[i] = tokens
    for copy in copies[2:]:
        copy.wait()


def project(x_ref, gain_ref, q_ref, k_ref, v_ref, g_ref, out_ref, half_ref):
    x = x_ref[...].astype(F32).reshape(-1, x_ref.shape[2]).T
    normed = (x * gain_ref[...].reshape(1, -1)).astype(BF16)
    at = 0
    for w_ref in (q_ref, k_ref, v_ref, g_ref):
        store_rows(out_ref, jnp.dot(normed, w_ref[...], preferred_element_type=F32), at)
        at += w_ref.shape[1]
    squares = jnp.sum(x * x, axis=1, keepdims=True)
    store_rows(out_ref, jnp.broadcast_to(squares, (x.shape[0], LANES)), at)
    core = lax.axis_index("core")
    width = half_ref.shape[1]
    half_ref[...] = jnp.where(core == 0, x[:, :width], x[:, width:]).astype(BF16)


def frequencies(shape):
    lane = lax.broadcasted_iota(jnp.int32, shape, 1)
    result = jnp.ones(shape, F32)
    for bit in range(6):
        factor = 10000.0 ** (-(2.0**bit) / (QK // 2))
        result = jnp.where((lane >> bit) & 1 == 1, result * F32(factor), result)
    return result


def sine_cosine(angle):
    turns = jnp.floor(angle * F32(2.0 / math.pi) + 0.5)
    rest = angle - turns * F32(1.5703125)
    rest = rest - turns * F32(4.837512969970703125e-4)
    rest = rest - turns * F32(7.54978995489188216e-8)
    square = rest * rest
    sine = rest + rest * square * (
        F32(-1.6666654611e-1) + square * (F32(8.3321608736e-3) + square * F32(-1.9515295891e-4))
    )
    cosine = (
        1.0
        - 0.5 * square
        + square
        * square
        * (
            F32(4.166664568298827e-2)
            + square * (F32(-1.388731625493765e-3) + square * F32(2.443315711809948e-5))
        )
    )
    quarter = turns.astype(jnp.int32) & 3
    odd = (quarter & 1) == 1
    first, second = jnp.where(odd, cosine, sine), jnp.where(odd, sine, cosine)
    return (
        jnp.where(quarter >= 2, -first, first),
        jnp.where((quarter == 1) | (quarter == 2), -second, second),
    )


def retain(parts_ref, sine_ref, cosine_ref, state_ref, out_ref, new_ref):
    sums = summed(parts_ref)
    rows = sums.shape[0]
    scale = lax.rsqrt(sums[:, 2 * QK + 2 * VD :] / D + 1e-06)
    wide_scale = jnp.concatenate([scale, scale], axis=1)
    signed, cosine = sine_ref[...], cosine_ref[...]

    def rotated(vectors):
        return vectors * cosine + pltpu.roll(vectors, QK // 2, 1) * signed

    query = rotated(sums[:, :QK] * scale).astype(BF16).astype(F32)
    key = (rotated(sums[:, QK : 2 * QK] * scale) * QK ** (-0.5)).astype(BF16).astype(F32)
    value = (sums[:, 2 * QK : 2 * QK + VD] * wide_scale).astype(BF16).astype(F32)
    gate = sums[:, 2 * QK + VD : 2 * QK + 2 * VD] * wide_scale
    columns = jnp.concatenate([query, key] * (QK // (2 * rows)), axis=0).T
    head = jnp.full((1, VD), tp_index(), jnp.int32).astype(F32)
    decay = 1.0 - jnp.exp2(-5.0 - 10.0 * head / (HEADS - 1))
    retained = []
    for i in range(rows):
        state = (
            decay * state_ref[i, 0]
            + columns[:, rows + i : rows + i + 1] * value[i : i + 1]
        )
        new_ref[i, 0] = state
        retained.append(jnp.sum(state * columns[:, i : i + 1], axis=0, keepdims=True))
    retained = jnp.concatenate(retained, axis=0)
    inverse = lax.rsqrt(jnp.mean(retained * retained, axis=1, keepdims=True) + 1e-06)
    merged = (retained * inverse * (gate / (1.0 + jnp.exp(-gate)))).astype(BF16)
    for i in range(out_ref.shape[0]):
        out_ref[i] = merged


def write_out(value_ref, out_ref, sem):
    copy = pltpu.make_async_copy(value_ref, out_ref, sem)
    copy.start()
    copy.wait()


def mix(merged_ref, own_ref, other_ref, out_ref):
    core = lax.axis_index("core")
    half = out_ref.shape[2]
    total = None
    for w_ref, which in ((own_ref, core), (other_ref, 1 - core)):
        merged = jnp.concatenate(
            [merged_ref[i + which].astype(F32) for i in range(0, merged_ref.shape[0], 2)], axis=0
        )
        weight = jnp.where(core == 0, w_ref[:, :half], w_ref[:, half:])
        part = jnp.dot(merged.astype(BF16), weight, preferred_element_type=F32)
        total = part if total is None else total + part
    total = total.astype(BF16)
    for i in range(out_ref.shape[0]):
        out_ref[i] = total


def add_chips(parts_ref, token_ref, *refs):
    out_ref = refs[-1]
    out_ref[...] = (token_ref[...].astype(F32) + summed(parts_ref)).astype(BF16)


def expand(half_ref, other_ref, gain_ref, gate_ref, up_ref, out_ref, mine_ref):
    me = tp_index()
    first = lax.axis_index("core") == 0
    half, other = half_ref[...].astype(F32), other_ref[...].astype(F32)
    x = jnp.concatenate(
        [jnp.where(first, half, other), jnp.where(first, other, half)], axis=1
    )
    normed = (x * gain_ref[...].reshape(1, -1)).astype(BF16)
    contract = (((1,), (1,)), ((), ()))
    units = gate_ref.shape[0]
    gate = lax.dot_general(normed, gate_ref[...], contract, preferred_element_type=F32)
    up = lax.dot_general(normed, up_ref[...], contract, preferred_element_type=F32)
    spare = out_ref.shape[2] // 2 - units
    squares = jnp.broadcast_to(jnp.sum(x * x, axis=1, keepdims=True), (x.shape[0], spare))
    store_rows(out_ref, jnp.concatenate([gate, squares, up, squares], axis=1), 0)
    shape = (mine_ref.shape[0], x.shape[1])
    row = lax.broadcasted_iota(jnp.int32, shape, 0)
    pick = lax.broadcasted_iota(jnp.int32, shape, 1) == row + me * shape[0]
    mine_ref[...] = lax.dot_general(
        pick.astype(BF16), x.astype(BF16), contract, preferred_element_type=F32
    )


def activate(parts_ref, out_ref):
    sums = summed(parts_ref)
    units, middle = out_ref.shape[2], sums.shape[1] // 2
    scale = lax.rsqrt(sums[:, units : units + 1] / D + 1e-06)
    gate = sums[:, :units] * scale
    up = sums[:, middle : middle + units] * scale
    hidden = (gate / (1.0 + jnp.exp(-gate)) * up).astype(BF16)
    for i in range(out_ref.shape[0]):
        out_ref[i] = hidden


def contract_units(hidden_ref, w_ref, out_ref):
    down = jnp.dot(all_rows(hidden_ref).astype(BF16), w_ref[...], preferred_element_type=F32)
    out_ref[...] = down.T.astype(BF16).reshape(out_ref.shape)


def finish(parts_ref, mine_ref, out_ref):
    out_ref[...] = (mine_ref[...] + summed(parts_ref)).astype(BF16)


def exchanged(blocks, axis, groups=None):
    return lax.all_to_all(blocks, axis, 0, 0, tiled=True, axis_index_groups=groups)


def on_device(
    tokens,
    lengths,
    retention_state,
    mixer_gain,
    query_weight,
    key_weight,
    value_weight,
    gate_weight,
    output_weight,
    channel_gain,
    ffn_gate,
    ffn_up,
    ffn_down,
):
    owners, chips, cores = (lax.axis_size(a) for a in ("kv", "z", "core"))
    members = chips * cores
    batch, own_width = tokens.shape
    rows = batch // owners
    half = own_width * members // cores
    units = ffn_gate.shape[1]
    middle = -(-(units + 1) // LANES) * LANES
    swap = [(0, 1), (1, 0)]
    gate_rows, up_rows = ffn_gate.T, ffn_up.T
    along_z = [[0, 1, 4, 3, 2, 5, 7, 6]] if chips == 8 else None
    along_kv = [list(kv_order(owners))]

    weights = (query_weight, key_weight, value_weight, gate_weight)
    fetch = (mixer_gain, channel_gain, *weights)
    copies, sine, cosine, mixer_gain, channel_gain, *weights = local_call(
        prepare,
        (
            shaped((members, own_width, batch), BF16),
            shaped((rows, QK), F32),
            shaped((rows, QK), F32),
            *(shaped(a.shape, a.dtype) for a in fetch),
        ),
        tokens.T,
        lengths,
        *fetch,
        scratch=(
            pltpu.VMEM((own_width, batch), BF16),
            pltpu.SMEM((rows,), jnp.int32),
            pltpu.SemaphoreType.DMA((len(fetch) + 2,)),
        ),
        space=pltpu.HBM,
        limit=FULL_VMEM_BYTES,
    )
    other_weight = lax.ppermute(output_weight, "core", swap)
    features = exchanged(copies, ("z", "core"))
    features, other_weight = lax.optimization_barrier((features, other_weight))
    width = 2 * QK + 2 * VD + LANES
    parts, token_half = local_call(
        project,
        (shaped((owners, rows, width), BF16), shaped((batch, half), BF16)),
        features,
        mixer_gain,
        *weights,
    )
    merged, new_state = local_call(
        retain,
        (shaped((owners * cores, rows, VD), BF16), shaped(retention_state.shape, F32)),
        exchanged(parts, "kv", along_kv),
        sine,
        cosine,
        retention_state,
    )
    chip_sum = local_call(
        mix,
        shaped((chips, batch, half), BF16),
        exchanged(merged, ("kv", "core")),
        output_weight,
        other_weight,
    )
    residual_half = local_call(
        add_chips,
        shaped((batch, half), BF16),
        exchanged(chip_sum, "z", along_z),
        token_half,
        gate_rows,
        up_rows,
    )
    residual_other = lax.ppermute(residual_half, "core", swap)
    new_state, _ = lax.optimization_barrier((new_state, residual_half))
    new_state = local_call(
        write_out,
        jax.ShapeDtypeStruct(retention_state.shape, F32),
        new_state,
        scratch=(pltpu.SemaphoreType.DMA,),
        out_space=pl.ANY,
    )
    residual_other, new_state = lax.optimization_barrier((residual_other, new_state))
    parts, mine = local_call(
        expand,
        (shaped((owners, rows, 2 * middle), BF16), shaped((own_width, batch), F32)),
        residual_half,
        residual_other,
        channel_gain,
        gate_rows,
        up_rows,
    )
    hidden = local_call(
        activate, shaped((owners, rows, units), BF16), exchanged(parts, "kv", along_kv)
    )
    down = local_call(
        contract_units,
        shaped((members, own_width, batch), BF16),
        exchanged(hidden, "kv", along_kv),
        ffn_down,
    )
    layer_output = local_call(
        finish, jax.ShapeDtypeStruct((own_width, batch), BF16), exchanged(down, ("z", "core")), mine
    )
    return (layer_output.T, new_state)


def solution(mesh):
    split = Mesh(
        mesh.devices.reshape(mesh.shape["kv"], mesh.shape["tp"] // 2, 2), ("kv", "z", "core")
    )
    tp = ("z", "core")
    in_specs = (
        P(None, ("kv", *tp)),
        P("kv"),
        P("kv", tp, None, None),
        P("kv"),
        P("kv", tp),
        P("kv", tp),
        P("kv", tp),
        P("kv", tp),
        P(tp, "kv"),
        P("kv"),
        P("kv", tp),
        P("kv", tp),
        P(tp, "kv"),
    )
    out_specs = (P(None, ("kv", *tp)), P("kv", tp, None, None))
    return jax.shard_map(
        on_device, mesh=split, in_specs=in_specs, out_specs=out_specs, check_vma=False
    )
```

```python
import math

import jax
import jax.numpy as jnp
from jax import lax
from jax.experimental import pallas as pl
from jax.experimental.pallas import tpu as pltpu
from jax.sharding import Mesh, PartitionSpec as P

D = 4096
HEADS = 16
QK = 128
VD = 256
LANES = 128
KV_ORDER = (0, 8, 15, 14, 5, 2, 3, 11, 6, 13, 10, 4, 9, 7, 1, 12)
F32 = jnp.float32
BF16 = jnp.bfloat16
VMEM_BYTES = 8 << 20
LONG = pl.CostEstimate(flops=4_000_000_000, bytes_accessed=8_000_000, transcendentals=0)
FULL_VMEM_BYTES = 67_043_328 - 1_000_000


def local_call(kernel, outs, *operands, scratch=(), space=pltpu.VMEM, out_space=pltpu.VMEM, limit=VMEM_BYTES, cost=None):
    spaces = [space] * len(operands)
    several = isinstance(outs, tuple)
    vmem = pl.BlockSpec(memory_space=out_space)
    return pl.pallas_call(
        kernel,
        out_shape=outs,
        in_specs=[pl.BlockSpec(memory_space=s) for s in spaces],
        out_specs=tuple(vmem for _ in outs) if several else vmem,
        scratch_shapes=scratch,
        cost_estimate=cost,
        compiler_params=pltpu.CompilerParams(vmem_limit_bytes=limit),
    )(*operands)


def tp_index():
    return lax.axis_index("z") * lax.axis_size("core") + lax.axis_index("core")


def shaped(shape, dtype):
    return pltpu.VMEM(shape, dtype)


def kv_order(owners):
    return KV_ORDER if owners == len(KV_ORDER) else tuple(range(owners))


def store_rows(out_ref, value, start):
    each = out_ref.shape[1]
    for at, owner in enumerate(kv_order(out_ref.shape[0])):
        out_ref[at, :, start : start + value.shape[1]] = value[
            owner * each : (owner + 1) * each
        ].astype(out_ref.dtype)


def all_rows(ref):
    order = kv_order(ref.shape[0])
    return jnp.concatenate(
        [ref[order.index(owner)].astype(F32) for owner in range(ref.shape[0])], axis=0
    )


def summed(ref):
    total = ref[0].astype(F32)
    for i in range(1, ref.shape[0]):
        total = total + ref[i].astype(F32)
    return total


def prepare(token_ref, length_ref, *refs):
    count = (len(refs) - 5) // 2
    sources, (tokens_vmem, sine_ref, cosine_ref), fetched = (
        refs[:count],
        refs[count : count + 3],
        refs[count + 3 : 2 * count + 3],
    )
    lengths_smem, sems = refs[2 * count + 3 :]
    copies = [
        pltpu.make_async_copy(source, target, sems.at[i])
        for i, (source, target) in enumerate(
            zip((length_ref, token_ref, *sources), (lengths_smem, tokens_vmem, *fetched))
        )
    ]
    for copy in copies:
        copy.start()
    copies[0].wait()
    shape = sine_ref.shape
    row = lax.broadcasted_iota(jnp.int32, shape, 0)
    position = jnp.zeros(shape, F32)
    for i in range(shape[0]):
        position = jnp.where(row == i, lengths_smem[i].astype(F32), position)
    sine, cosine = sine_cosine(position * frequencies(shape))
    first = lax.broadcasted_iota(jnp.int32, shape, 1) < QK // 2
    sine_ref[...] = jnp.where(first, -sine, sine)
    cosine_ref[...] = cosine
    for copy in copies[1:]:
        copy.wait()


def spread(token_ref, out_ref):
    tokens = token_ref[...]
    for i in range(out_ref.shape[0]):
        out_ref[i] = tokens


def project(x_ref, gain_ref, q_ref, k_ref, v_ref, g_ref, out_ref, half_ref):
    x = x_ref[...].astype(F32).reshape(-1, x_ref.shape[2]).T
    normed = (x * gain_ref[...].reshape(1, -1)).astype(BF16)
    at = 0
    for w_ref in (q_ref, k_ref, v_ref, g_ref):
        store_rows(out_ref, jnp.dot(normed, w_ref[...], preferred_element_type=F32), at)
        at += w_ref.shape[1]
    squares = jnp.sum(x * x, axis=1, keepdims=True)
    store_rows(out_ref, jnp.broadcast_to(squares, (x.shape[0], LANES)), at)
    core = lax.axis_index("core")
    width = half_ref.shape[1]
    half_ref[...] = jnp.where(core == 0, x[:, :width], x[:, width:]).astype(BF16)


def frequencies(shape):
    lane = lax.broadcasted_iota(jnp.int32, shape, 1)
    result = jnp.ones(shape, F32)
    for bit in range(6):
        factor = 10000.0 ** (-(2.0**bit) / (QK // 2))
        result = jnp.where((lane >> bit) & 1 == 1, result * F32(factor), result)
    return result


def sine_cosine(angle):
    turns = jnp.floor(angle * F32(2.0 / math.pi) + 0.5)
    rest = angle - turns * F32(1.5703125)
    rest = rest - turns * F32(4.837512969970703125e-4)
    rest = rest - turns * F32(7.54978995489188216e-8)
    square = rest * rest
    sine = rest + rest * square * (
        F32(-1.6666654611e-1) + square * (F32(8.3321608736e-3) + square * F32(-1.9515295891e-4))
    )
    cosine = (
        1.0
        - 0.5 * square
        + square
        * square
        * (
            F32(4.166664568298827e-2)
            + square * (F32(-1.388731625493765e-3) + square * F32(2.443315711809948e-5))
        )
    )
    quarter = turns.astype(jnp.int32) & 3
    odd = (quarter & 1) == 1
    first, second = jnp.where(odd, cosine, sine), jnp.where(odd, sine, cosine)
    return (
        jnp.where(quarter >= 2, -first, first),
        jnp.where((quarter == 1) | (quarter == 2), -second, second),
    )


def retain(parts_ref, sine_ref, cosine_ref, state_ref, out_ref, new_ref):
    sums = summed(parts_ref)
    rows = sums.shape[0]
    scale = lax.rsqrt(sums[:, 2 * QK + 2 * VD :] / D + 1e-06)
    wide_scale = jnp.concatenate([scale, scale], axis=1)
    signed, cosine = sine_ref[...], cosine_ref[...]

    def rotated(vectors):
        return vectors * cosine + pltpu.roll(vectors, QK // 2, 1) * signed

    query = rotated(sums[:, :QK] * scale).astype(BF16).astype(F32)
    key = (rotated(sums[:, QK : 2 * QK] * scale) * QK ** (-0.5)).astype(BF16).astype(F32)
    value = (sums[:, 2 * QK : 2 * QK + VD] * wide_scale).astype(BF16).astype(F32)
    gate = sums[:, 2 * QK + VD : 2 * QK + 2 * VD] * wide_scale
    columns = jnp.concatenate([query, key] * (QK // (2 * rows)), axis=0).T
    head = jnp.full((1, VD), tp_index(), jnp.int32).astype(F32)
    decay = 1.0 - jnp.exp2(-5.0 - 10.0 * head / (HEADS - 1))
    retained = []
    for i in range(rows):
        state = (
            decay * state_ref[i, 0]
            + columns[:, rows + i : rows + i + 1] * value[i : i + 1]
        )
        new_ref[i, 0] = state
        retained.append(jnp.sum(state * columns[:, i : i + 1], axis=0, keepdims=True))
    retained = jnp.concatenate(retained, axis=0)
    inverse = lax.rsqrt(jnp.mean(retained * retained, axis=1, keepdims=True) + 1e-06)
    merged = (retained * inverse * (gate / (1.0 + jnp.exp(-gate)))).astype(BF16)
    for i in range(out_ref.shape[0]):
        out_ref[i] = merged


def write_out(value_ref, out_ref, sem):
    copy = pltpu.make_async_copy(value_ref, out_ref, sem)
    copy.start()
    copy.wait()


def mix(merged_ref, own_ref, other_ref, out_ref):
    core = lax.axis_index("core")
    half = out_ref.shape[2]
    total = None
    for w_ref, which in ((own_ref, core), (other_ref, 1 - core)):
        merged = jnp.concatenate(
            [merged_ref[i + which].astype(F32) for i in range(0, merged_ref.shape[0], 2)], axis=0
        )
        weight = jnp.where(core == 0, w_ref[:, :half], w_ref[:, half:])
        part = jnp.dot(merged.astype(BF16), weight, preferred_element_type=F32)
        total = part if total is None else total + part
    total = total.astype(BF16)
    for i in range(out_ref.shape[0]):
        out_ref[i] = total


def add_chips(parts_ref, token_ref, *refs):
    out_ref = refs[-1]
    out_ref[...] = (token_ref[...].astype(F32) + summed(parts_ref)).astype(BF16)


def expand(half_ref, other_ref, gain_ref, gate_ref, up_ref, out_ref, mine_ref):
    me = tp_index()
    first = lax.axis_index("core") == 0
    half, other = half_ref[...].astype(F32), other_ref[...].astype(F32)
    x = jnp.concatenate(
        [jnp.where(first, half, other), jnp.where(first, other, half)], axis=1
    )
    normed = (x * gain_ref[...].reshape(1, -1)).astype(BF16)
    contract = (((1,), (1,)), ((), ()))
    units = gate_ref.shape[0]
    gate = lax.dot_general(normed, gate_ref[...], contract, preferred_element_type=F32)
    up = lax.dot_general(normed, up_ref[...], contract, preferred_element_type=F32)
    spare = out_ref.shape[2] // 2 - units
    squares = jnp.broadcast_to(jnp.sum(x * x, axis=1, keepdims=True), (x.shape[0], spare))
    store_rows(out_ref, jnp.concatenate([gate, squares, up, squares], axis=1), 0)
    shape = (mine_ref.shape[0], x.shape[1])
    row = lax.broadcasted_iota(jnp.int32, shape, 0)
    pick = lax.broadcasted_iota(jnp.int32, shape, 1) == row + me * shape[0]
    mine_ref[...] = lax.dot_general(
        pick.astype(BF16), x.astype(BF16), contract, preferred_element_type=F32
    )


def activate(parts_ref, out_ref):
    sums = summed(parts_ref)
    units, middle = out_ref.shape[2], sums.shape[1] // 2
    scale = lax.rsqrt(sums[:, units : units + 1] / D + 1e-06)
    gate = sums[:, :units] * scale
    up = sums[:, middle : middle + units] * scale
    hidden = (gate / (1.0 + jnp.exp(-gate)) * up).astype(BF16)
    for i in range(out_ref.shape[0]):
        out_ref[i] = hidden


def contract_units(hidden_ref, w_ref, out_ref):
    down = jnp.dot(all_rows(hidden_ref).astype(BF16), w_ref[...], preferred_element_type=F32)
    out_ref[...] = down.T.astype(BF16).reshape(out_ref.shape)


def finish(parts_ref, mine_ref, out_ref):
    out_ref[...] = (mine_ref[...] + summed(parts_ref)).astype(BF16)


def exchanged(blocks, axis, groups=None):
    return lax.all_to_all(blocks, axis, 0, 0, tiled=True, axis_index_groups=groups)


def on_device(
    tokens,
    lengths,
    retention_state,
    mixer_gain,
    query_weight,
    key_weight,
    value_weight,
    gate_weight,
    output_weight,
    channel_gain,
    ffn_gate,
    ffn_up,
    ffn_down,
):
    owners, chips, cores = (lax.axis_size(a) for a in ("kv", "z", "core"))
    members = chips * cores
    batch, own_width = tokens.shape
    rows = batch // owners
    half = own_width * members // cores
    units = ffn_gate.shape[1]
    middle = -(-(units + 1) // LANES) * LANES
    swap = [(0, 1), (1, 0)]
    gate_rows, up_rows = ffn_gate.T, ffn_up.T
    along_z = [[0, 1, 4, 3, 2, 5, 7, 6]] if chips == 8 else None
    along_kv = [list(kv_order(owners))]

    weights = (query_weight, key_weight, value_weight, gate_weight)
    own, sine, cosine, mixer_gain, channel_gain = local_call(
        prepare,
        (
            shaped((own_width, batch), BF16),
            shaped((rows, QK), F32),
            shaped((rows, QK), F32),
            shaped(mixer_gain.shape, F32),
            shaped(channel_gain.shape, F32),
        ),
        tokens.T,
        lengths,
        mixer_gain,
        channel_gain,
        scratch=(
            pltpu.SMEM((rows,), jnp.int32),
            pltpu.SemaphoreType.DMA((4,)),
        ),
        space=pltpu.HBM,
        limit=FULL_VMEM_BYTES,
    )
    copies = local_call(
        spread, shaped((members, own_width, batch), BF16), own, cost=LONG
    )
    other_weight = lax.ppermute(output_weight, "core", swap)
    features = exchanged(copies, ("z", "core"))
    features, other_weight = lax.optimization_barrier((features, other_weight))
    width = 2 * QK + 2 * VD + LANES
    parts, token_half = local_call(
        project,
        (shaped((owners, rows, width), BF16), shaped((batch, half), BF16)),
        features,
        mixer_gain,
        *weights,
    )
    merged, new_state = local_call(
        retain,
        (shaped((owners * cores, rows, VD), BF16), shaped(retention_state.shape, F32)),
        exchanged(parts, "kv", along_kv),
        sine,
        cosine,
        retention_state,
    )
    chip_sum = local_call(
        mix,
        shaped((chips, batch, half), BF16),
        exchanged(merged, ("kv", "core")),
        output_weight,
        other_weight,
    )
    residual_half = local_call(
        add_chips,
        shaped((batch, half), BF16),
        exchanged(chip_sum, "z", along_z),
        token_half,
        gate_rows,
        up_rows,
    )
    residual_other = lax.ppermute(residual_half, "core", swap)
    new_state, _ = lax.optimization_barrier((new_state, residual_half))
    new_state = local_call(
        write_out,
        jax.ShapeDtypeStruct(retention_state.shape, F32),
        new_state,
        scratch=(pltpu.SemaphoreType.DMA,),
        out_space=pl.ANY,
    )
    residual_other, new_state = lax.optimization_barrier((residual_other, new_state))
    parts, mine = local_call(
        expand,
        (shaped((owners, rows, 2 * middle), BF16), shaped((own_width, batch), F32)),
        residual_half,
        residual_other,
        channel_gain,
        gate_rows,
        up_rows,
    )
    hidden = local_call(
        activate, shaped((owners, rows, units), BF16), exchanged(parts, "kv", along_kv)
    )
    down = local_call(
        contract_units,
        shaped((members, own_width, batch), BF16),
        exchanged(hidden, "kv", along_kv),
        ffn_down,
    )
    layer_output = local_call(
        finish, jax.ShapeDtypeStruct((own_width, batch), BF16), exchanged(down, ("z", "core")), mine
    )
    return (layer_output.T, new_state)


def solution(mesh):
    split = Mesh(
        mesh.devices.reshape(mesh.shape["kv"], mesh.shape["tp"] // 2, 2), ("kv", "z", "core")
    )
    tp = ("z", "core")
    in_specs = (
        P(None, ("kv", *tp)),
        P("kv"),
        P("kv", tp, None, None),
        P("kv"),
        P("kv", tp),
        P("kv", tp),
        P("kv", tp),
        P("kv", tp),
        P(tp, "kv"),
        P("kv"),
        P("kv", tp),
        P("kv", tp),
        P(tp, "kv"),
    )
    out_specs = (P(None, ("kv", *tp)), P("kv", tp, None, None))
    return jax.shard_map(
        on_device, mesh=split, in_specs=in_specs, out_specs=out_specs, check_vma=False
    )
```

```python
import math

import jax
import jax.numpy as jnp
from jax import lax
from jax.experimental import pallas as pl
from jax.experimental.pallas import tpu as pltpu
from jax.sharding import Mesh, PartitionSpec as P

D = 4096
HEADS = 16
QK = 128
VD = 256
LANES = 128
TP_ORDER = (1, 0, 2, 3, 4, 5, 6, 7, 8, 9, 10, 11, 12, 13, 14, 15)
KV_ORDER = (0, 8, 15, 14, 5, 2, 3, 11, 6, 13, 10, 4, 9, 7, 1, 12)
F32 = jnp.float32
BF16 = jnp.bfloat16
VMEM_BYTES = 8 << 20
LONG = pl.CostEstimate(flops=4_000_000_000, bytes_accessed=8_000_000, transcendentals=0)
FULL_VMEM_BYTES = 67_043_328 - 1_000_000


def local_call(kernel, outs, *operands, scratch=(), space=pltpu.VMEM, out_space=pltpu.VMEM, limit=VMEM_BYTES, cost=None):
    spaces = [space] * len(operands)
    several = isinstance(outs, tuple)
    vmem = pl.BlockSpec(memory_space=out_space)
    return pl.pallas_call(
        kernel,
        out_shape=outs,
        in_specs=[pl.BlockSpec(memory_space=s) for s in spaces],
        out_specs=tuple(vmem for _ in outs) if several else vmem,
        scratch_shapes=scratch,
        cost_estimate=cost,
        compiler_params=pltpu.CompilerParams(vmem_limit_bytes=limit),
    )(*operands)


def tp_index():
    return lax.axis_index("z") * lax.axis_size("core") + lax.axis_index("core")


def shaped(shape, dtype):
    return pltpu.VMEM(shape, dtype)


def kv_order(owners):
    return KV_ORDER if owners == len(KV_ORDER) else tuple(range(owners))


def tp_order(members):
    return TP_ORDER if members == len(TP_ORDER) else tuple(range(members))


def store_rows(out_ref, value, start):
    each = out_ref.shape[1]
    for at, owner in enumerate(kv_order(out_ref.shape[0])):
        out_ref[at, :, start : start + value.shape[1]] = value[
            owner * each : (owner + 1) * each
        ].astype(out_ref.dtype)


def all_rows(ref):
    order = kv_order(ref.shape[0])
    return jnp.concatenate(
        [ref[order.index(owner)].astype(F32) for owner in range(ref.shape[0])], axis=0
    )


def summed(ref):
    total = ref[0].astype(F32)
    for i in range(1, ref.shape[0]):
        total = total + ref[i].astype(F32)
    return total


def prepare(token_ref, length_ref, *refs):
    count = (len(refs) - 5) // 2
    sources, (tokens_vmem, sine_ref, cosine_ref), fetched = (
        refs[:count],
        refs[count : count + 3],
        refs[count + 3 : 2 * count + 3],
    )
    lengths_smem, sems = refs[2 * count + 3 :]
    copies = [
        pltpu.make_async_copy(source, target, sems.at[i])
        for i, (source, target) in enumerate(
            zip((length_ref, token_ref, *sources), (lengths_smem, tokens_vmem, *fetched))
        )
    ]
    for copy in copies:
        copy.start()
    copies[0].wait()
    shape = sine_ref.shape
    row = lax.broadcasted_iota(jnp.int32, shape, 0)
    position = jnp.zeros(shape, F32)
    for i in range(shape[0]):
        position = jnp.where(row == i, lengths_smem[i].astype(F32), position)
    sine, cosine = sine_cosine(position * frequencies(shape))
    first = lax.broadcasted_iota(jnp.int32, shape, 1) < QK // 2
    sine_ref[...] = jnp.where(first, -sine, sine)
    cosine_ref[...] = cosine
    for copy in copies[1:]:
        copy.wait()


def spread(token_ref, out_ref):
    tokens = token_ref[...]
    for i in range(out_ref.shape[0]):
        out_ref[i] = tokens


def project(x_ref, gain_ref, q_ref, k_ref, v_ref, g_ref, out_ref, half_ref):
    x = x_ref[...].astype(F32).reshape(-1, x_ref.shape[2]).T
    normed = (x * gain_ref[...].reshape(1, -1)).astype(BF16)
    at = 0
    for w_ref in (q_ref, k_ref, v_ref, g_ref):
        store_rows(out_ref, jnp.dot(normed, w_ref[...], preferred_element_type=F32), at)
        at += w_ref.shape[1]
    squares = jnp.sum(x * x, axis=1, keepdims=True)
    store_rows(out_ref, jnp.broadcast_to(squares, (x.shape[0], LANES)), at)
    core = lax.axis_index("core")
    width = half_ref.shape[1]
    half_ref[...] = jnp.where(core == 0, x[:, :width], x[:, width:]).astype(BF16)


def frequencies(shape):
    lane = lax.broadcasted_iota(jnp.int32, shape, 1)
    result = jnp.ones(shape, F32)
    for bit in range(6):
        factor = 10000.0 ** (-(2.0**bit) / (QK // 2))
        result = jnp.where((lane >> bit) & 1 == 1, result * F32(factor), result)
    return result


def sine_cosine(angle):
    turns = jnp.floor(angle * F32(2.0 / math.pi) + 0.5)
    rest = angle - turns * F32(1.5703125)
    rest = rest - turns * F32(4.837512969970703125e-4)
    rest = rest - turns * F32(7.54978995489188216e-8)
    square = rest * rest
    sine = rest + rest * square * (
        F32(-1.6666654611e-1) + square * (F32(8.3321608736e-3) + square * F32(-1.9515295891e-4))
    )
    cosine = (
        1.0
        - 0.5 * square
        + square
        * square
        * (
            F32(4.166664568298827e-2)
            + square * (F32(-1.388731625493765e-3) + square * F32(2.443315711809948e-5))
        )
    )
    quarter = turns.astype(jnp.int32) & 3
    odd = (quarter & 1) == 1
    first, second = jnp.where(odd, cosine, sine), jnp.where(odd, sine, cosine)
    return (
        jnp.where(quarter >= 2, -first, first),
        jnp.where((quarter == 1) | (quarter == 2), -second, second),
    )


def retain(parts_ref, sine_ref, cosine_ref, state_ref, out_ref, new_ref):
    sums = summed(parts_ref)
    rows = sums.shape[0]
    scale = lax.rsqrt(sums[:, 2 * QK + 2 * VD :] / D + 1e-06)
    wide_scale = jnp.concatenate([scale, scale], axis=1)
    signed, cosine = sine_ref[...], cosine_ref[...]

    def rotated(vectors):
        return vectors * cosine + pltpu.roll(vectors, QK // 2, 1) * signed

    query = rotated(sums[:, :QK] * scale).astype(BF16).astype(F32)
    key = (rotated(sums[:, QK : 2 * QK] * scale) * QK ** (-0.5)).astype(BF16).astype(F32)
    value = (sums[:, 2 * QK : 2 * QK + VD] * wide_scale).astype(BF16).astype(F32)
    gate = sums[:, 2 * QK + VD : 2 * QK + 2 * VD] * wide_scale
    columns = jnp.concatenate([query, key] * (QK // (2 * rows)), axis=0).T
    head = jnp.full((1, VD), tp_index(), jnp.int32).astype(F32)
    decay = 1.0 - jnp.exp2(-5.0 - 10.0 * head / (HEADS - 1))
    retained = []
    for i in range(rows):
        state = (
            decay * state_ref[i, 0]
            + columns[:, rows + i : rows + i + 1] * value[i : i + 1]
        )
        new_ref[i, 0] = state
        retained.append(jnp.sum(state * columns[:, i : i + 1], axis=0, keepdims=True))
    retained = jnp.concatenate(retained, axis=0)
    inverse = lax.rsqrt(jnp.mean(retained * retained, axis=1, keepdims=True) + 1e-06)
    merged = (retained * inverse * (gate / (1.0 + jnp.exp(-gate)))).astype(BF16)
    for i in range(out_ref.shape[0]):
        out_ref[i] = merged


def write_out(value_ref, out_ref, sem):
    copy = pltpu.make_async_copy(value_ref, out_ref, sem)
    copy.start()
    copy.wait()


def mix(merged_ref, own_ref, other_ref, out_ref):
    core = lax.axis_index("core")
    half = out_ref.shape[2]
    total = None
    for w_ref, which in ((own_ref, core), (other_ref, 1 - core)):
        merged = jnp.concatenate(
            [merged_ref[i + which].astype(F32) for i in range(0, merged_ref.shape[0], 2)], axis=0
        )
        weight = jnp.where(core == 0, w_ref[:, :half], w_ref[:, half:])
        part = jnp.dot(merged.astype(BF16), weight, preferred_element_type=F32)
        total = part if total is None else total + part
    total = total.astype(BF16)
    for i in range(out_ref.shape[0]):
        out_ref[i] = total


def add_chips(parts_ref, token_ref, *refs):
    out_ref = refs[-1]
    out_ref[...] = (token_ref[...].astype(F32) + summed(parts_ref)).astype(BF16)


def expand(half_ref, other_ref, gain_ref, gate_ref, up_ref, out_ref, mine_ref):
    me = tp_index()
    first = lax.axis_index("core") == 0
    half, other = half_ref[...].astype(F32), other_ref[...].astype(F32)
    x = jnp.concatenate(
        [jnp.where(first, half, other), jnp.where(first, other, half)], axis=1
    )
    normed = (x * gain_ref[...].reshape(1, -1)).astype(BF16)
    contract = (((1,), (1,)), ((), ()))
    units = gate_ref.shape[0]
    gate = lax.dot_general(normed, gate_ref[...], contract, preferred_element_type=F32)
    up = lax.dot_general(normed, up_ref[...], contract, preferred_element_type=F32)
    spare = out_ref.shape[2] // 2 - units
    squares = jnp.broadcast_to(jnp.sum(x * x, axis=1, keepdims=True), (x.shape[0], spare))
    store_rows(out_ref, jnp.concatenate([gate, squares, up, squares], axis=1), 0)
    shape = (mine_ref.shape[0], x.shape[1])
    row = lax.broadcasted_iota(jnp.int32, shape, 0)
    pick = lax.broadcasted_iota(jnp.int32, shape, 1) == row + me * shape[0]
    mine_ref[...] = lax.dot_general(
        pick.astype(BF16), x.astype(BF16), contract, preferred_element_type=F32
    )


def activate(parts_ref, out_ref):
    sums = summed(parts_ref)
    units, middle = out_ref.shape[2], sums.shape[1] // 2
    scale = lax.rsqrt(sums[:, units : units + 1] / D + 1e-06)
    gate = sums[:, :units] * scale
    up = sums[:, middle : middle + units] * scale
    hidden = (gate / (1.0 + jnp.exp(-gate)) * up).astype(BF16)
    for i in range(out_ref.shape[0]):
        out_ref[i] = hidden


def contract_units(hidden_ref, w_ref, out_ref):
    down = jnp.dot(all_rows(hidden_ref).astype(BF16), w_ref[...], preferred_element_type=F32)
    down = down.T.astype(BF16)
    each = out_ref.shape[1]
    for at, owner in enumerate(tp_order(out_ref.shape[0])):
        out_ref[at] = down[owner * each : (owner + 1) * each]


def finish(parts_ref, mine_ref, out_ref):
    out_ref[...] = (mine_ref[...] + summed(parts_ref)).astype(BF16)


def exchanged(blocks, axis, groups=None):
    return lax.all_to_all(blocks, axis, 0, 0, tiled=True, axis_index_groups=groups)


def on_device(
    tokens,
    lengths,
    retention_state,
    mixer_gain,
    query_weight,
    key_weight,
    value_weight,
    gate_weight,
    output_weight,
    channel_gain,
    ffn_gate,
    ffn_up,
    ffn_down,
):
    owners, chips, cores = (lax.axis_size(a) for a in ("kv", "z", "core"))
    members = chips * cores
    batch, own_width = tokens.shape
    rows = batch // owners
    half = own_width * members // cores
    units = ffn_gate.shape[1]
    middle = -(-(units + 1) // LANES) * LANES
    swap = [(0, 1), (1, 0)]
    gate_rows, up_rows = ffn_gate.T, ffn_up.T
    along_z = [[0, 1, 4, 3, 2, 5, 7, 6]] if chips == 8 else None
    along_kv = [list(kv_order(owners))]

    weights = (query_weight, key_weight, value_weight, gate_weight)
    own, sine, cosine, mixer_gain, channel_gain = local_call(
        prepare,
        (
            shaped((own_width, batch), BF16),
            shaped((rows, QK), F32),
            shaped((rows, QK), F32),
            shaped(mixer_gain.shape, F32),
            shaped(channel_gain.shape, F32),
        ),
        tokens.T,
        lengths,
        mixer_gain,
        channel_gain,
        scratch=(
            pltpu.SMEM((rows,), jnp.int32),
            pltpu.SemaphoreType.DMA((4,)),
        ),
        space=pltpu.HBM,
        limit=FULL_VMEM_BYTES,
    )
    copies = local_call(
        spread, shaped((members, own_width, batch), BF16), own, cost=LONG
    )
    other_weight = lax.ppermute(output_weight, "core", swap)
    features = exchanged(copies, ("z", "core"))
    features, other_weight = lax.optimization_barrier((features, other_weight))
    width = 2 * QK + 2 * VD + LANES
    parts, token_half = local_call(
        project,
        (shaped((owners, rows, width), BF16), shaped((batch, half), BF16)),
        features,
        mixer_gain,
        *weights,
    )
    merged, new_state = local_call(
        retain,
        (shaped((owners * cores, rows, VD), BF16), shaped(retention_state.shape, F32)),
        exchanged(parts, "kv", along_kv),
        sine,
        cosine,
        retention_state,
    )
    chip_sum = local_call(
        mix,
        shaped((chips, batch, half), BF16),
        exchanged(merged, ("kv", "core")),
        output_weight,
        other_weight,
    )
    residual_half = local_call(
        add_chips,
        shaped((batch, half), BF16),
        exchanged(chip_sum, "z", along_z),
        token_half,
        gate_rows,
        up_rows,
    )
    residual_other = lax.ppermute(residual_half, "core", swap)
    new_state, _ = lax.optimization_barrier((new_state, residual_half))
    new_state = local_call(
        write_out,
        jax.ShapeDtypeStruct(retention_state.shape, F32),
        new_state,
        scratch=(pltpu.SemaphoreType.DMA,),
        out_space=pl.ANY,
    )
    residual_other, new_state = lax.optimization_barrier((residual_other, new_state))
    parts, mine = local_call(
        expand,
        (shaped((owners, rows, 2 * middle), BF16), shaped((own_width, batch), F32)),
        residual_half,
        residual_other,
        channel_gain,
        gate_rows,
        up_rows,
    )
    hidden = local_call(
        activate, shaped((owners, rows, units), BF16), exchanged(parts, "kv", along_kv)
    )
    down = local_call(
        contract_units,
        shaped((members, own_width, batch), BF16),
        exchanged(hidden, "kv", along_kv),
        ffn_down,
    )
    layer_output = local_call(
        finish, jax.ShapeDtypeStruct((own_width, batch), BF16), exchanged(down, ("z", "core"), [list(tp_order(members))]), mine
    )
    return (layer_output.T, new_state)


def solution(mesh):
    split = Mesh(
        mesh.devices.reshape(mesh.shape["kv"], mesh.shape["tp"] // 2, 2), ("kv", "z", "core")
    )
    tp = ("z", "core")
    in_specs = (
        P(None, ("kv", *tp)),
        P("kv"),
        P("kv", tp, None, None),
        P("kv"),
        P("kv", tp),
        P("kv", tp),
        P("kv", tp),
        P("kv", tp),
        P(tp, "kv"),
        P("kv"),
        P("kv", tp),
        P("kv", tp),
        P(tp, "kv"),
    )
    out_specs = (P(None, ("kv", *tp)), P("kv", tp, None, None))
    return jax.shard_map(
        on_device, mesh=split, in_specs=in_specs, out_specs=out_specs, check_vma=False
    )
```

```python
import math

import jax
import jax.numpy as jnp
from jax import lax
from jax.experimental import pallas as pl
from jax.experimental.pallas import tpu as pltpu
from jax.sharding import Mesh, PartitionSpec as P

D = 4096
HEADS = 16
QK = 128
VD = 256
LANES = 128
TP_ORDER = (1, 0, 2, 3, 4, 5, 6, 7, 8, 9, 10, 11, 12, 13, 14, 15)
KV_ORDER = (0, 8, 15, 14, 5, 2, 3, 11, 6, 13, 10, 4, 9, 7, 1, 12)
F32 = jnp.float32
BF16 = jnp.bfloat16
VMEM_BYTES = 8 << 20
LONG = pl.CostEstimate(flops=4_000_000_000, bytes_accessed=8_000_000, transcendentals=0)
FULL_VMEM_BYTES = 67_043_328 - 1_000_000


def local_call(kernel, outs, *operands, scratch=(), space=pltpu.VMEM, out_space=pltpu.VMEM, limit=VMEM_BYTES, cost=None):
    spaces = [space] * len(operands)
    several = isinstance(outs, tuple)
    vmem = pl.BlockSpec(memory_space=out_space)
    return pl.pallas_call(
        kernel,
        out_shape=outs,
        in_specs=[pl.BlockSpec(memory_space=s) for s in spaces],
        out_specs=tuple(vmem for _ in outs) if several else vmem,
        scratch_shapes=scratch,
        cost_estimate=cost,
        compiler_params=pltpu.CompilerParams(vmem_limit_bytes=limit),
    )(*operands)


def tp_index():
    return lax.axis_index("z") * lax.axis_size("core") + lax.axis_index("core")


def shaped(shape, dtype):
    return pltpu.VMEM(shape, dtype)


def kv_order(owners):
    return KV_ORDER if owners == len(KV_ORDER) else tuple(range(owners))


def tp_order(members):
    return TP_ORDER if members == len(TP_ORDER) else tuple(range(members))


def store_rows(out_ref, value, start):
    each = out_ref.shape[1]
    for at, owner in enumerate(kv_order(out_ref.shape[0])):
        out_ref[at, :, start : start + value.shape[1]] = value[
            owner * each : (owner + 1) * each
        ].astype(out_ref.dtype)


def all_rows(ref):
    order = kv_order(ref.shape[0])
    return jnp.concatenate(
        [ref[order.index(owner)].astype(F32) for owner in range(ref.shape[0])], axis=0
    )


def summed(ref):
    total = ref[0].astype(F32)
    for i in range(1, ref.shape[0]):
        total = total + ref[i].astype(F32)
    return total


def prepare(token_ref, length_ref, *refs):
    count = (len(refs) - 5) // 2
    sources, (tokens_vmem, sine_ref, cosine_ref), fetched = (
        refs[:count],
        refs[count : count + 3],
        refs[count + 3 : 2 * count + 3],
    )
    lengths_smem, sems = refs[2 * count + 3 :]
    copies = [
        pltpu.make_async_copy(source, target, sems.at[i])
        for i, (source, target) in enumerate(
            zip((length_ref, token_ref, *sources), (lengths_smem, tokens_vmem, *fetched))
        )
    ]
    for copy in copies:
        copy.start()
    copies[0].wait()
    shape = sine_ref.shape
    row = lax.broadcasted_iota(jnp.int32, shape, 0)
    position = jnp.zeros(shape, F32)
    for i in range(shape[0]):
        position = jnp.where(row == i, lengths_smem[i].astype(F32), position)
    sine, cosine = sine_cosine(position * frequencies(shape))
    first = lax.broadcasted_iota(jnp.int32, shape, 1) < QK // 2
    sine_ref[...] = jnp.where(first, -sine, sine)
    cosine_ref[...] = cosine
    for copy in copies[1:]:
        copy.wait()


def spread(token_ref, out_ref):
    tokens = token_ref[...]
    for i in range(out_ref.shape[0]):
        out_ref[i] = tokens


def project(x_ref, gain_ref, q_ref, k_ref, v_ref, g_ref, out_ref, half_ref):
    x = x_ref[...].astype(F32).reshape(-1, x_ref.shape[2]).T
    normed = (x * gain_ref[...].reshape(1, -1)).astype(BF16)
    at = 0
    for w_ref in (q_ref, k_ref, v_ref, g_ref):
        store_rows(out_ref, jnp.dot(normed, w_ref[...], preferred_element_type=F32), at)
        at += w_ref.shape[1]
    squares = jnp.sum(x * x, axis=1, keepdims=True)
    store_rows(out_ref, jnp.broadcast_to(squares, (x.shape[0], LANES)), at)
    core = lax.axis_index("core")
    width = half_ref.shape[1]
    half_ref[...] = jnp.where(core == 0, x[:, :width], x[:, width:]).astype(BF16)


def frequencies(shape):
    lane = lax.broadcasted_iota(jnp.int32, shape, 1)
    result = jnp.ones(shape, F32)
    for bit in range(6):
        factor = 10000.0 ** (-(2.0**bit) / (QK // 2))
        result = jnp.where((lane >> bit) & 1 == 1, result * F32(factor), result)
    return result


def sine_cosine(angle):
    turns = jnp.floor(angle * F32(2.0 / math.pi) + 0.5)
    rest = angle - turns * F32(1.5703125)
    rest = rest - turns * F32(4.837512969970703125e-4)
    rest = rest - turns * F32(7.54978995489188216e-8)
    square = rest * rest
    sine = rest + rest * square * (
        F32(-1.6666654611e-1) + square * (F32(8.3321608736e-3) + square * F32(-1.9515295891e-4))
    )
    cosine = (
        1.0
        - 0.5 * square
        + square
        * square
        * (
            F32(4.166664568298827e-2)
            + square * (F32(-1.388731625493765e-3) + square * F32(2.443315711809948e-5))
        )
    )
    quarter = turns.astype(jnp.int32) & 3
    odd = (quarter & 1) == 1
    first, second = jnp.where(odd, cosine, sine), jnp.where(odd, sine, cosine)
    return (
        jnp.where(quarter >= 2, -first, first),
        jnp.where((quarter == 1) | (quarter == 2), -second, second),
    )


def retain(parts_ref, sine_ref, cosine_ref, state_ref, out_ref, new_ref):
    sums = summed(parts_ref)
    rows = sums.shape[0]
    scale = lax.rsqrt(sums[:, 2 * QK + 2 * VD :] / D + 1e-06)
    wide_scale = jnp.concatenate([scale, scale], axis=1)
    signed, cosine = sine_ref[...], cosine_ref[...]

    def rotated(vectors):
        return vectors * cosine + pltpu.roll(vectors, QK // 2, 1) * signed

    query = rotated(sums[:, :QK] * scale).astype(BF16).astype(F32)
    key = (rotated(sums[:, QK : 2 * QK] * scale) * QK ** (-0.5)).astype(BF16).astype(F32)
    value = (sums[:, 2 * QK : 2 * QK + VD] * wide_scale).astype(BF16).astype(F32)
    gate = sums[:, 2 * QK + VD : 2 * QK + 2 * VD] * wide_scale
    columns = jnp.concatenate([query, key] * (QK // (2 * rows)), axis=0).T
    head = jnp.full((1, VD), tp_index(), jnp.int32).astype(F32)
    decay = 1.0 - jnp.exp2(-5.0 - 10.0 * head / (HEADS - 1))
    retained = []
    for i in range(rows):
        state = (
            decay * state_ref[i, 0]
            + columns[:, rows + i : rows + i + 1] * value[i : i + 1]
        )
        new_ref[i, 0] = state
        retained.append(jnp.sum(state * columns[:, i : i + 1], axis=0, keepdims=True))
    retained = jnp.concatenate(retained, axis=0)
    inverse = lax.rsqrt(jnp.mean(retained * retained, axis=1, keepdims=True) + 1e-06)
    merged = (retained * inverse * (gate / (1.0 + jnp.exp(-gate)))).astype(BF16)
    for i in range(out_ref.shape[0]):
        out_ref[i] = merged


def write_out(value_ref, out_ref, sem):
    copy = pltpu.make_async_copy(value_ref, out_ref, sem)
    copy.start()
    copy.wait()


def mix(merged_ref, own_ref, other_ref, out_ref):
    core = lax.axis_index("core")
    half = out_ref.shape[2]
    total = None
    for w_ref, which in ((own_ref, core), (other_ref, 1 - core)):
        merged = jnp.concatenate(
            [merged_ref[i + which].astype(F32) for i in range(0, merged_ref.shape[0], 2)], axis=0
        )
        weight = jnp.where(core == 0, w_ref[:, :half], w_ref[:, half:])
        part = jnp.dot(merged.astype(BF16), weight, preferred_element_type=F32)
        total = part if total is None else total + part
    total = total.astype(BF16)
    for i in range(out_ref.shape[0]):
        out_ref[i] = total


def add_chips(parts_ref, token_ref, *refs):
    out_ref = refs[-1]
    out_ref[...] = (token_ref[...].astype(F32) + summed(parts_ref)).astype(BF16)


def expand(half_ref, other_ref, gain_ref, gate_ref, up_ref, out_ref, mine_ref):
    me = tp_index()
    first = lax.axis_index("core") == 0
    half, other = half_ref[...].astype(F32), other_ref[...].astype(F32)
    x = jnp.concatenate(
        [jnp.where(first, half, other), jnp.where(first, other, half)], axis=1
    )
    normed = (x * gain_ref[...].reshape(1, -1)).astype(BF16)
    contract = (((1,), (1,)), ((), ()))
    units = gate_ref.shape[0]
    gate = lax.dot_general(normed, gate_ref[...], contract, preferred_element_type=F32)
    up = lax.dot_general(normed, up_ref[...], contract, preferred_element_type=F32)
    spare = out_ref.shape[2] // 2 - units
    squares = jnp.broadcast_to(jnp.sum(x * x, axis=1, keepdims=True), (x.shape[0], spare))
    store_rows(out_ref, jnp.concatenate([gate, squares, up, squares], axis=1), 0)
    shape = (mine_ref.shape[0], x.shape[1])
    row = lax.broadcasted_iota(jnp.int32, shape, 0)
    pick = lax.broadcasted_iota(jnp.int32, shape, 1) == row + me * shape[0]
    mine_ref[...] = lax.dot_general(
        pick.astype(BF16), x.astype(BF16), contract, preferred_element_type=F32
    )


def activate(parts_ref, out_ref):
    sums = summed(parts_ref)
    units, middle = out_ref.shape[2], sums.shape[1] // 2
    scale = lax.rsqrt(sums[:, units : units + 1] / D + 1e-06)
    gate = sums[:, :units] * scale
    up = sums[:, middle : middle + units] * scale
    hidden = (gate / (1.0 + jnp.exp(-gate)) * up).astype(BF16)
    for i in range(out_ref.shape[0]):
        out_ref[i] = hidden


def contract_units(hidden_ref, w_ref, out_ref):
    down = jnp.dot(all_rows(hidden_ref).astype(BF16), w_ref[...], preferred_element_type=F32)
    down = down.T.astype(BF16)
    each = out_ref.shape[1]
    for at, owner in enumerate(tp_order(out_ref.shape[0])):
        out_ref[at] = down[owner * each : (owner + 1) * each]


def finish(parts_ref, mine_ref, out_ref):
    out_ref[...] = (mine_ref[...] + summed(parts_ref)).astype(BF16)


def exchanged(blocks, axis, groups=None):
    return lax.all_to_all(blocks, axis, 0, 0, tiled=True, axis_index_groups=groups)


def on_device(
    tokens,
    lengths,
    retention_state,
    mixer_gain,
    query_weight,
    key_weight,
    value_weight,
    gate_weight,
    output_weight,
    channel_gain,
    ffn_gate,
    ffn_up,
    ffn_down,
):
    owners, chips, cores = (lax.axis_size(a) for a in ("kv", "z", "core"))
    members = chips * cores
    batch, own_width = tokens.shape
    rows = batch // owners
    half = own_width * members // cores
    units = ffn_gate.shape[1]
    middle = -(-(units + 1) // LANES) * LANES
    swap = [(0, 1), (1, 0)]
    gate_rows, up_rows = ffn_gate.T, ffn_up.T
    along_z = [[3 * i % chips for i in range(chips)]]
    along_kv = [list(kv_order(owners))]

    weights = (query_weight, key_weight, value_weight, gate_weight)
    own, sine, cosine, mixer_gain, channel_gain = local_call(
        prepare,
        (
            shaped((own_width, batch), BF16),
            shaped((rows, QK), F32),
            shaped((rows, QK), F32),
            shaped(mixer_gain.shape, F32),
            shaped(channel_gain.shape, F32),
        ),
        tokens.T,
        lengths,
        mixer_gain,
        channel_gain,
        scratch=(
            pltpu.SMEM((rows,), jnp.int32),
            pltpu.SemaphoreType.DMA((4,)),
        ),
        space=pltpu.HBM,
        limit=FULL_VMEM_BYTES,
    )
    copies = local_call(
        spread, shaped((members, own_width, batch), BF16), own, cost=LONG
    )
    other_weight = lax.ppermute(output_weight, "core", swap)
    features = exchanged(copies, ("z", "core"))
    features, other_weight = lax.optimization_barrier((features, other_weight))
    width = 2 * QK + 2 * VD + LANES
    parts, token_half = local_call(
        project,
        (shaped((owners, rows, width), BF16), shaped((batch, half), BF16)),
        features,
        mixer_gain,
        *weights,
    )
    merged, new_state = local_call(
        retain,
        (shaped((owners * cores, rows, VD), BF16), shaped(retention_state.shape, F32)),
        exchanged(parts, "kv", along_kv),
        sine,
        cosine,
        retention_state,
    )
    chip_sum = local_call(
        mix,
        shaped((chips, batch, half), BF16),
        exchanged(merged, ("kv", "core")),
        output_weight,
        other_weight,
    )
    residual_half = local_call(
        add_chips,
        shaped((batch, half), BF16),
        exchanged(chip_sum, "z", along_z),
        token_half,
        gate_rows,
        up_rows,
    )
    residual_other = lax.ppermute(residual_half, "core", swap)
    new_state, _ = lax.optimization_barrier((new_state, residual_half))
    new_state = local_call(
        write_out,
        jax.ShapeDtypeStruct(retention_state.shape, F32),
        new_state,
        scratch=(pltpu.SemaphoreType.DMA,),
        out_space=pl.ANY,
    )
    residual_other, new_state = lax.optimization_barrier((residual_other, new_state))
    parts, mine = local_call(
        expand,
        (shaped((owners, rows, 2 * middle), BF16), shaped((own_width, batch), F32)),
        residual_half,
        residual_other,
        channel_gain,
        gate_rows,
        up_rows,
    )
    hidden = local_call(
        activate, shaped((owners, rows, units), BF16), exchanged(parts, "kv", along_kv)
    )
    down = local_call(
        contract_units,
        shaped((members, own_width, batch), BF16),
        exchanged(hidden, "kv", along_kv),
        ffn_down,
    )
    layer_output = local_call(
        finish, jax.ShapeDtypeStruct((own_width, batch), BF16), exchanged(down, ("z", "core"), [list(tp_order(members))]), mine
    )
    return (layer_output.T, new_state)


def solution(mesh):
    split = Mesh(
        mesh.devices.reshape(mesh.shape["kv"], mesh.shape["tp"] // 2, 2), ("kv", "z", "core")
    )
    tp = ("z", "core")
    in_specs = (
        P(None, ("kv", *tp)),
        P("kv"),
        P("kv", tp, None, None),
        P("kv"),
        P("kv", tp),
        P("kv", tp),
        P("kv", tp),
        P("kv", tp),
        P(tp, "kv"),
        P("kv"),
        P("kv", tp),
        P("kv", tp),
        P(tp, "kv"),
    )
    out_specs = (P(None, ("kv", *tp)), P("kv", tp, None, None))
    return jax.shard_map(
        on_device, mesh=split, in_specs=in_specs, out_specs=out_specs, check_vma=False
    )
```

```python
import math

import jax
import jax.numpy as jnp
from jax import lax
from jax.experimental import pallas as pl
from jax.experimental.pallas import tpu as pltpu
from jax.sharding import Mesh, PartitionSpec as P

D = 4096
HEADS = 16
QK = 128
VD = 256
LANES = 128
TP_ORDER = (1, 0, 2, 3, 4, 5, 6, 7, 8, 9, 10, 11, 12, 13, 14, 15)
KV_ORDER = (0, 8, 15, 14, 5, 2, 3, 11, 6, 13, 10, 4, 9, 7, 1, 12)
F32 = jnp.float32
BF16 = jnp.bfloat16
VMEM_BYTES = 8 << 20
LONG = pl.CostEstimate(flops=4_000_000_000, bytes_accessed=8_000_000, transcendentals=0)
FULL_VMEM_BYTES = 67_043_328 - 1_000_000


def local_call(kernel, outs, *operands, scratch=(), space=pltpu.VMEM, out_space=pltpu.VMEM, limit=VMEM_BYTES, cost=None):
    spaces = [space] * len(operands)
    several = isinstance(outs, tuple)
    vmem = pl.BlockSpec(memory_space=out_space)
    return pl.pallas_call(
        kernel,
        out_shape=outs,
        in_specs=[pl.BlockSpec(memory_space=s) for s in spaces],
        out_specs=tuple(vmem for _ in outs) if several else vmem,
        scratch_shapes=scratch,
        cost_estimate=cost,
        compiler_params=pltpu.CompilerParams(vmem_limit_bytes=limit),
    )(*operands)


def tp_index():
    return lax.axis_index("z") * lax.axis_size("core") + lax.axis_index("core")


def shaped(shape, dtype):
    return pltpu.VMEM(shape, dtype)


def kv_order(owners):
    return KV_ORDER if owners == len(KV_ORDER) else tuple(range(owners))


def tp_order(members):
    return TP_ORDER if members == len(TP_ORDER) else tuple(range(members))


def store_rows(out_ref, value, start):
    each = out_ref.shape[1]
    for at, owner in enumerate(kv_order(out_ref.shape[0])):
        out_ref[at, :, start : start + value.shape[1]] = value[
            owner * each : (owner + 1) * each
        ].astype(out_ref.dtype)


def all_rows(ref):
    order = kv_order(ref.shape[0])
    return jnp.concatenate(
        [ref[order.index(owner)].astype(F32) for owner in range(ref.shape[0])], axis=0
    )


def summed(ref):
    total = ref[0].astype(F32)
    for i in range(1, ref.shape[0]):
        total = total + ref[i].astype(F32)
    return total


def prepare(token_ref, length_ref, *refs):
    count = (len(refs) - 5) // 2
    sources, (tokens_vmem, sine_ref, cosine_ref), fetched = (
        refs[:count],
        refs[count : count + 3],
        refs[count + 3 : 2 * count + 3],
    )
    lengths_smem, sems = refs[2 * count + 3 :]
    copies = [
        pltpu.make_async_copy(source, target, sems.at[i])
        for i, (source, target) in enumerate(
            zip((length_ref, token_ref, *sources), (lengths_smem, tokens_vmem, *fetched))
        )
    ]
    for copy in copies:
        copy.start()
    copies[0].wait()
    shape = sine_ref.shape
    row = lax.broadcasted_iota(jnp.int32, shape, 0)
    position = jnp.zeros(shape, F32)
    for i in range(shape[0]):
        position = jnp.where(row == i, lengths_smem[i].astype(F32), position)
    sine, cosine = sine_cosine(position * frequencies(shape))
    first = lax.broadcasted_iota(jnp.int32, shape, 1) < QK // 2
    sine_ref[...] = jnp.where(first, -sine, sine)
    cosine_ref[...] = cosine
    for copy in copies[1:]:
        copy.wait()


def spread(token_ref, out_ref):
    tokens = token_ref[...]
    for i in range(out_ref.shape[0]):
        out_ref[i] = tokens


def project(x_ref, gain_ref, q_ref, k_ref, v_ref, g_ref, out_ref, half_ref):
    x = x_ref[...].astype(F32).reshape(-1, x_ref.shape[2]).T
    normed = (x * gain_ref[...].reshape(1, -1)).astype(BF16)
    at = 0
    for w_ref in (q_ref, k_ref, v_ref, g_ref):
        store_rows(out_ref, jnp.dot(normed, w_ref[...], preferred_element_type=F32), at)
        at += w_ref.shape[1]
    squares = jnp.sum(x * x, axis=1, keepdims=True)
    store_rows(out_ref, jnp.broadcast_to(squares, (x.shape[0], LANES)), at)
    core = lax.axis_index("core")
    width = half_ref.shape[1]
    half_ref[...] = jnp.where(core == 0, x[:, :width], x[:, width:]).astype(BF16)


def frequencies(shape):
    lane = lax.broadcasted_iota(jnp.int32, shape, 1)
    result = jnp.ones(shape, F32)
    for bit in range(6):
        factor = 10000.0 ** (-(2.0**bit) / (QK // 2))
        result = jnp.where((lane >> bit) & 1 == 1, result * F32(factor), result)
    return result


def sine_cosine(angle):
    turns = jnp.floor(angle * F32(2.0 / math.pi) + 0.5)
    rest = angle - turns * F32(1.5703125)
    rest = rest - turns * F32(4.837512969970703125e-4)
    rest = rest - turns * F32(7.54978995489188216e-8)
    square = rest * rest
    sine = rest + rest * square * (
        F32(-1.6666654611e-1) + square * (F32(8.3321608736e-3) + square * F32(-1.9515295891e-4))
    )
    cosine = (
        1.0
        - 0.5 * square
        + square
        * square
        * (
            F32(4.166664568298827e-2)
            + square * (F32(-1.388731625493765e-3) + square * F32(2.443315711809948e-5))
        )
    )
    quarter = turns.astype(jnp.int32) & 3
    odd = (quarter & 1) == 1
    first, second = jnp.where(odd, cosine, sine), jnp.where(odd, sine, cosine)
    return (
        jnp.where(quarter >= 2, -first, first),
        jnp.where((quarter == 1) | (quarter == 2), -second, second),
    )


def retain(parts_ref, sine_ref, cosine_ref, state_ref, out_ref, new_ref):
    sums = summed(parts_ref)
    rows = sums.shape[0]
    scale = lax.rsqrt(sums[:, 2 * QK + 2 * VD :] / D + 1e-06)
    wide_scale = jnp.concatenate([scale, scale], axis=1)
    signed, cosine = sine_ref[...], cosine_ref[...]

    def rotated(vectors):
        return vectors * cosine + pltpu.roll(vectors, QK // 2, 1) * signed

    query = rotated(sums[:, :QK] * scale).astype(BF16).astype(F32)
    key = (rotated(sums[:, QK : 2 * QK] * scale) * QK ** (-0.5)).astype(BF16).astype(F32)
    value = (sums[:, 2 * QK : 2 * QK + VD] * wide_scale).astype(BF16).astype(F32)
    gate = sums[:, 2 * QK + VD : 2 * QK + 2 * VD] * wide_scale
    columns = jnp.concatenate([query, key] * (QK // (2 * rows)), axis=0).T
    head = jnp.full((1, VD), tp_index(), jnp.int32).astype(F32)
    decay = 1.0 - jnp.exp2(-5.0 - 10.0 * head / (HEADS - 1))
    retained = []
    for i in range(rows):
        state = (
            decay * state_ref[i, 0]
            + columns[:, rows + i : rows + i + 1] * value[i : i + 1]
        )
        new_ref[i, 0] = state
        retained.append(jnp.sum(state * columns[:, i : i + 1], axis=0, keepdims=True))
    retained = jnp.concatenate(retained, axis=0)
    inverse = lax.rsqrt(jnp.mean(retained * retained, axis=1, keepdims=True) + 1e-06)
    merged = (retained * inverse * (gate / (1.0 + jnp.exp(-gate)))).astype(BF16)
    for i in range(out_ref.shape[0]):
        out_ref[i] = merged


def write_out(value_ref, out_ref, sem):
    copy = pltpu.make_async_copy(value_ref, out_ref, sem)
    copy.start()
    copy.wait()


def mix(merged_ref, own_ref, other_ref, out_ref):
    core = lax.axis_index("core")
    half = out_ref.shape[2]
    total = None
    for w_ref, which in ((own_ref, core), (other_ref, 1 - core)):
        merged = jnp.concatenate(
            [merged_ref[i + which].astype(F32) for i in range(0, merged_ref.shape[0], 2)], axis=0
        )
        weight = w_ref[:, pl.ds(pl.multiple_of(core * half, half), half)]
        part = jnp.dot(merged.astype(BF16), weight, preferred_element_type=F32)
        total = part if total is None else total + part
    total = total.astype(BF16)
    for i in range(out_ref.shape[0]):
        out_ref[i] = total


def add_chips(parts_ref, token_ref, *refs):
    out_ref = refs[-1]
    out_ref[...] = (token_ref[...].astype(F32) + summed(parts_ref)).astype(BF16)


def expand(half_ref, other_ref, gain_ref, gate_ref, up_ref, out_ref, mine_ref):
    me = tp_index()
    first = lax.axis_index("core") == 0
    half, other = half_ref[...].astype(F32), other_ref[...].astype(F32)
    x = jnp.concatenate(
        [jnp.where(first, half, other), jnp.where(first, other, half)], axis=1
    )
    normed = (x * gain_ref[...].reshape(1, -1)).astype(BF16)
    contract = (((1,), (1,)), ((), ()))
    units = gate_ref.shape[0]
    gate = lax.dot_general(normed, gate_ref[...], contract, preferred_element_type=F32)
    up = lax.dot_general(normed, up_ref[...], contract, preferred_element_type=F32)
    spare = out_ref.shape[2] // 2 - units
    squares = jnp.broadcast_to(jnp.sum(x * x, axis=1, keepdims=True), (x.shape[0], spare))
    store_rows(out_ref, jnp.concatenate([gate, squares, up, squares], axis=1), 0)
    shape = (mine_ref.shape[0], x.shape[1])
    row = lax.broadcasted_iota(jnp.int32, shape, 0)
    pick = lax.broadcasted_iota(jnp.int32, shape, 1) == row + me * shape[0]
    mine_ref[...] = lax.dot_general(
        pick.astype(BF16), x.astype(BF16), contract, preferred_element_type=F32
    )


def activate(parts_ref, out_ref):
    sums = summed(parts_ref)
    units, middle = out_ref.shape[2], sums.shape[1] // 2
    scale = lax.rsqrt(sums[:, units : units + 1] / D + 1e-06)
    gate = sums[:, :units] * scale
    up = sums[:, middle : middle + units] * scale
    hidden = (gate / (1.0 + jnp.exp(-gate)) * up).astype(BF16)
    for i in range(out_ref.shape[0]):
        out_ref[i] = hidden


def contract_units(hidden_ref, w_ref, out_ref):
    down = jnp.dot(all_rows(hidden_ref).astype(BF16), w_ref[...], preferred_element_type=F32)
    down = down.T.astype(BF16)
    each = out_ref.shape[1]
    for at, owner in enumerate(tp_order(out_ref.shape[0])):
        out_ref[at] = down[owner * each : (owner + 1) * each]


def finish(parts_ref, mine_ref, out_ref):
    out_ref[...] = (mine_ref[...] + summed(parts_ref)).astype(BF16)


def exchanged(blocks, axis, groups=None):
    return lax.all_to_all(blocks, axis, 0, 0, tiled=True, axis_index_groups=groups)


def on_device(
    tokens,
    lengths,
    retention_state,
    mixer_gain,
    query_weight,
    key_weight,
    value_weight,
    gate_weight,
    output_weight,
    channel_gain,
    ffn_gate,
    ffn_up,
    ffn_down,
):
    owners, chips, cores = (lax.axis_size(a) for a in ("kv", "z", "core"))
    members = chips * cores
    batch, own_width = tokens.shape
    rows = batch // owners
    half = own_width * members // cores
    units = ffn_gate.shape[1]
    middle = -(-(units + 1) // LANES) * LANES
    swap = [(0, 1), (1, 0)]
    gate_rows, up_rows = ffn_gate.T, ffn_up.T
    along_z = [[0, 1, 4, 3, 2, 5, 7, 6]] if chips == 8 else None
    along_kv = [list(kv_order(owners))]

    weights = (query_weight, key_weight, value_weight, gate_weight)
    own, sine, cosine, mixer_gain, channel_gain = local_call(
        prepare,
        (
            shaped((own_width, batch), BF16),
            shaped((rows, QK), F32),
            shaped((rows, QK), F32),
            shaped(mixer_gain.shape, F32),
            shaped(channel_gain.shape, F32),
        ),
        tokens.T,
        lengths,
        mixer_gain,
        channel_gain,
        scratch=(
            pltpu.SMEM((rows,), jnp.int32),
            pltpu.SemaphoreType.DMA((4,)),
        ),
        space=pltpu.HBM,
        limit=FULL_VMEM_BYTES,
    )
    copies = local_call(
        spread, shaped((members, own_width, batch), BF16), own, cost=LONG
    )
    other_weight = lax.ppermute(output_weight, "core", swap)
    features = exchanged(copies, ("z", "core"))
    features, other_weight = lax.optimization_barrier((features, other_weight))
    width = 2 * QK + 2 * VD + LANES
    parts, token_half = local_call(
        project,
        (shaped((owners, rows, width), BF16), shaped((batch, half), BF16)),
        features,
        mixer_gain,
        *weights,
    )
    merged, new_state = local_call(
        retain,
        (shaped((owners * cores, rows, VD), BF16), shaped(retention_state.shape, F32)),
        exchanged(parts, "kv", along_kv),
        sine,
        cosine,
        retention_state,
    )
    chip_sum = local_call(
        mix,
        shaped((chips, batch, half), BF16),
        exchanged(merged, ("kv", "core")),
        output_weight,
        other_weight,
    )
    residual_half = local_call(
        add_chips,
        shaped((batch, half), BF16),
        exchanged(chip_sum, "z", along_z),
        token_half,
        gate_rows,
        up_rows,
    )
    residual_other = lax.ppermute(residual_half, "core", swap)
    new_state, _ = lax.optimization_barrier((new_state, residual_half))
    new_state = local_call(
        write_out,
        jax.ShapeDtypeStruct(retention_state.shape, F32),
        new_state,
        scratch=(pltpu.SemaphoreType.DMA,),
        out_space=pl.ANY,
    )
    residual_other, new_state = lax.optimization_barrier((residual_other, new_state))
    parts, mine = local_call(
        expand,
        (shaped((owners, rows, 2 * middle), BF16), shaped((own_width, batch), F32)),
        residual_half,
        residual_other,
        channel_gain,
        gate_rows,
        up_rows,
    )
    hidden = local_call(
        activate, shaped((owners, rows, units), BF16), exchanged(parts, "kv", along_kv)
    )
    down = local_call(
        contract_units,
        shaped((members, own_width, batch), BF16),
        exchanged(hidden, "kv", along_kv),
        ffn_down,
    )
    layer_output = local_call(
        finish, jax.ShapeDtypeStruct((own_width, batch), BF16), exchanged(down, ("z", "core"), [list(tp_order(members))]), mine
    )
    return (layer_output.T, new_state)


def solution(mesh):
    split = Mesh(
        mesh.devices.reshape(mesh.shape["kv"], mesh.shape["tp"] // 2, 2), ("kv", "z", "core")
    )
    tp = ("z", "core")
    in_specs = (
        P(None, ("kv", *tp)),
        P("kv"),
        P("kv", tp, None, None),
        P("kv"),
        P("kv", tp),
        P("kv", tp),
        P("kv", tp),
        P("kv", tp),
        P(tp, "kv"),
        P("kv"),
        P("kv", tp),
        P("kv", tp),
        P(tp, "kv"),
    )
    out_specs = (P(None, ("kv", *tp)), P("kv", tp, None, None))
    return jax.shard_map(
        on_device, mesh=split, in_specs=in_specs, out_specs=out_specs, check_vma=False
    )
```
